1024 devices in a mesh: fs: 256 (over z, x, core), tp: 4 (over y).
Axes of the slice: x: 4, y: 4, z: 32, core: 2. Of those that a mesh axis runs over, the one named last changes fastest.
Arguments:
- normed_input: bfloat16 [131072, 2048], P('fs'), may hold values from -6 to 6
- value_cotangent: bfloat16 [131072, 2048], P('fs', 'tp'), may hold values from -6 to 6
- gated_output: bfloat16 [131072, 2048], P('fs', 'tp'), may hold values from -6 to 6
- layer_cotangent: bfloat16 [131072, 2048], P('fs'), may hold values from -6 to 6
- factor_value: bfloat16 [2048, 256], P('fs'), may hold values from -4 to 4, as said below
- factor_output: bfloat16 [2048, 256], P('fs'), may hold values from -4 to 4, as said below
- weight_value: float32 [2048, 2048], P('fs', 'tp'), may hold values from -0.125 to 0.125
- weight_output: float32 [2048, 2048], P('tp', 'fs'), may hold values from -0.125 to 0.125
- first_value: float32 [256, 2048], P('fs', 'tp'), may hold values from -8192 to 8192
- second_value: float32 [256, 2048], P('fs', 'tp'), may hold values from 524288 to 8388608
- first_output: float32 [256, 2048], P('fs', 'tp'), may hold values from -8192 to 8192
- second_output: float32 [256, 2048], P('fs', 'tp'), may hold values from 524288 to 8388608
Outputs:
- step_value: float32 [2048, 2048], P('fs', 'tp')
- step_output: float32 [2048, 2048], P('tp', 'fs')
- next_weight_value: float32 [2048, 2048], P('fs', 'tp')
- next_weight_output: float32 [2048, 2048], P('tp', 'fs')
- next_first_value: float32 [256, 2048], P('fs', 'tp')
- next_second_value: float32 [256, 2048], P('fs', 'tp')
- next_first_output: float32 [256, 2048], P('fs', 'tp')
- next_second_output: float32 [256, 2048], P('fs', 'tp')
- copy_value: bfloat16 [2048, 2048], P(None, 'tp')
- copy_output: bfloat16 [2048, 2048], P('tp')
The draws below stay inside these ranges and needn't reach their ends.
Inputs may be any that keep to these rules, and one draw needn't show every extreme that they name: factor_value has full rank. factor_output has full rank.
All inputs are finite; a program needn't handle non-finite values.
Results may differ from the reference program's by a relative error of at most 0.0039.
Values may be sent and summed in bfloat16 or wider, within the bound.
No kernel may reach another device: no remote copies, remote signals or barrier semaphores. Data moves between devices by JAX's collectives and lax.ppermute only.
A program may use at most 64 MiB of HBM per device.

```python
import math
import jax
import jax.numpy as jnp
from jax import lax

D = 2048
WIDTH = 2048
R = 256
TOKENS = 131072


def make_factor(key):
    rising = jnp.exp(jnp.log(10.0) * jnp.arange(D, dtype=jnp.float32) / D)
    base = jnp.clip(jax.random.normal(key, (D, R), jnp.float32), -6.0, 6.0)
    return (base * rising[:, None] / jnp.sqrt(jnp.float32(D))).astype(jnp.bfloat16)


def draw_factor_value(key, part):
    return make_factor(jax.random.fold_in(key, 11))


def draw_factor_output(key, part):
    return make_factor(jax.random.fold_in(key, 17))


def shard_levels(key, dims, split, low, high):
    gain, own = 1.0, jax.random.fold_in(key, 6)
    for position, parts in split:
        heights = jnp.exp(jax.random.uniform(jax.random.fold_in(own, position), (parts,), jnp.float32, low / len(split), high / len(split)))
        gain = gain * jnp.repeat(heights, dims[position] // parts).reshape([-1 if axis == position else 1 for axis in range(len(dims))])
    return gain


def scatter_about(own_key, shape, scale, limit, pieces=(), held_as=jnp.bfloat16):
    array = scale * jax.random.normal(own_key, shape, jnp.float32)
    if pieces:
        array = array * shard_levels(own_key, shape, pieces, -0.22, 0.18)
    return jnp.clip(array, -limit, limit).astype(held_as)


def setup_inputs(seed: int = 0) -> dict:
    keys = jax.random.split(jax.random.key(seed), 13)
    normed_input = scatter_about(keys[0], (TOKENS, D), 1.0, 6.0, ((0, 256),))
    value_cotangent = scatter_about(keys[1], (TOKENS, WIDTH), 1.0, 6.0, ((0, 256), (1, 4)))
    gated_output = scatter_about(keys[2], (TOKENS, WIDTH), 1.0, 6.0, ((0, 256), (1, 4)))
    layer_cotangent = scatter_about(keys[3], (TOKENS, D), 1.0, 6.0, ((0, 256),))
    factor_value = draw_factor_value(jax.random.fold_in(keys[12], 71), 0)
    factor_output = draw_factor_output(jax.random.fold_in(keys[12], 71), 0)
    weight_value = scatter_about(keys[6], (D, WIDTH), D ** -0.5, 0.125, ((0, 256), (1, 4)), jnp.float32)
    weight_output = scatter_about(keys[7], (WIDTH, D), WIDTH ** -0.5, 0.125, ((0, 4), (1, 256)), jnp.float32)
    first_value = scatter_about(keys[8], (R, WIDTH), (4 * TOKENS ** 0.5), 8192.0, ((0, 256), (1, 4)), jnp.float32)
    second_value = jnp.clip(jnp.exp(math.log(8388608) - 2.7725887 * jax.random.uniform(keys[9], (R, WIDTH), jnp.float32) ** shard_levels(keys[9], (R, WIDTH), ((0, 256), (1, 4)), -0.2, 0.2)), 524288.0, 8388608)
    first_output = scatter_about(keys[10], (R, WIDTH), (4 * TOKENS ** 0.5), 8192.0, ((0, 256), (1, 4)), jnp.float32)
    second_output = jnp.clip(jnp.exp(math.log(8388608) - 2.7725887 * jax.random.uniform(keys[11], (R, WIDTH), jnp.float32) ** shard_levels(keys[11], (R, WIDTH), ((0, 256), (1, 4)), -0.2, 0.2)), 524288.0, 8388608)
    return dict(normed_input=normed_input, value_cotangent=value_cotangent, gated_output=gated_output, layer_cotangent=layer_cotangent, factor_value=factor_value, factor_output=factor_output, weight_value=weight_value, weight_output=weight_output, first_value=first_value, second_value=second_value, first_output=first_output, second_output=second_output)


def reference(normed_input, value_cotangent, gated_output, layer_cotangent, factor_value, factor_output, weight_value, weight_output, first_value, second_value, first_output, second_output):
    projected_input = jnp.dot(normed_input, factor_value, preferred_element_type=jnp.float32).astype(jnp.bfloat16)
    projected_cotangent = jnp.dot(layer_cotangent, factor_output, preferred_element_type=jnp.float32).astype(jnp.bfloat16)
    low_value = jnp.dot(projected_input.T, value_cotangent, preferred_element_type=jnp.float32)
    low_output = jnp.dot(projected_cotangent.T, gated_output, preferred_element_type=jnp.float32)
    next_first_value = 0.9 * first_value + 0.1 * low_value
    next_second_value = 0.95 * second_value + 0.05 * low_value * low_value
    next_first_output = 0.9 * first_output + 0.1 * low_output
    next_second_output = 0.95 * second_output + 0.05 * low_output * low_output
    direction_value = (next_first_value * lax.rsqrt(next_second_value)).astype(jnp.bfloat16)
    direction_output = (next_first_output * lax.rsqrt(next_second_output)).astype(jnp.bfloat16)
    update_value = jnp.dot(factor_value, direction_value, preferred_element_type=jnp.float32)
    update_output = jnp.dot(direction_output.T, factor_output.T, preferred_element_type=jnp.float32)
    entries = D * WIDTH
    total_value = jnp.sum(update_value * update_value)
    total_output = jnp.sum(update_output * update_output)
    step_value = update_value * lax.rsqrt(total_value / entries + 1e-06)
    step_output = update_output * lax.rsqrt(total_output / entries + 1e-06)
    next_weight_value = weight_value - 0.02 * step_value
    next_weight_output = weight_output - 0.02 * step_output
    return (step_value, step_output, next_weight_value, next_weight_output, next_first_value, next_second_value, next_first_output, next_second_output, next_weight_value.astype(jnp.bfloat16), next_weight_output.astype(jnp.bfloat16))
```

```python
import jax
import jax.numpy as jnp
from jax import lax
from jax.sharding import Mesh
from jax.sharding import PartitionSpec as P

D = 2048
WIDTH = 2048
R = 256
FS = ("z", "x", "c")


def exchange(blocks, axes):
    return lax.all_to_all(blocks, axes, split_axis=0, concat_axis=0, tiled=True)


def to_all(block, axes):
    copies = jnp.broadcast_to(block[None], (lax.axis_size(axes), *block.shape))
    return exchange(copies, axes)


def body(
    normed_input,
    value_cotangent,
    gated_output,
    layer_cotangent,
    factor_value,
    factor_output,
    weight_value,
    weight_output,
    first_value,
    second_value,
    first_output,
    second_output,
):
    nz, nx, nc, ny = (lax.axis_size(a) for a in ("z", "x", "c", "tp"))
    rows = factor_value.shape[0]
    cols = value_cotangent.shape[1]
    quarter = lax.axis_index("tp")
    inner = (((0,), (0,)), ((), ()))

    half_value = weight_value.astype(jnp.bfloat16)
    half_output = weight_output.astype(jnp.bfloat16).T
    halves = jnp.concatenate([half_value, half_output], axis=1)
    with jax.named_scope("wz"):
        w = to_all(halves, "z")
    with jax.named_scope("wx"):
        w = to_all(w, "x")
    with jax.named_scope("wc"):
        w = to_all(w, "c")
    w = w.transpose(2, 1, 0, 3, 4).reshape(D, 2 * cols)

    place = jnp.arange(R).reshape(nz, nx * nc).T.reshape(R)
    turn = (jnp.arange(R)[:, None] == place[None, :]).astype(jnp.bfloat16)
    both = jnp.concatenate([factor_value, factor_output], axis=0)
    both = jnp.dot(both, turn, preferred_element_type=jnp.float32).astype(jnp.bfloat16)
    both = both.reshape(2, rows, 2, R // 2).transpose(0, 2, 1, 3).reshape(ny, rows, R // 2)
    mine = lax.dynamic_index_in_dim(both, quarter, 0, keepdims=False)
    with jax.named_scope("fz"):
        f = to_all(mine, "z")
    with jax.named_scope("fxy"):
        f = to_all(f, ("x", "tp"))
    with jax.named_scope("fc"):
        f = to_all(f, "c")
    f = f.reshape(nc, nx, 2, 2, nz, rows, R // 2).transpose(2, 4, 1, 0, 5, 3, 6).reshape(2, D, R)
    whole_value, whole_output = f[0], f[1]

    projected_input = jnp.dot(
        normed_input, whole_value, preferred_element_type=jnp.float32
    ).astype(jnp.bfloat16)
    projected_cotangent = jnp.dot(
        layer_cotangent, whole_output, preferred_element_type=jnp.float32
    ).astype(jnp.bfloat16)
    term_value = lax.dot_general(
        projected_input, value_cotangent, inner, preferred_element_type=jnp.float32
    )
    term_output = lax.dot_general(
        projected_cotangent, gated_output, inner, preferred_element_type=jnp.float32
    )
    terms = jnp.concatenate([term_value, term_output], axis=1).astype(jnp.bfloat16)
    with jax.named_scope("sxc"):
        t = exchange(terms.reshape(nx * nc, nz, 2 * cols), ("x", "c"))
    t = t.astype(jnp.float32).sum(axis=0).astype(jnp.bfloat16)
    with jax.named_scope("sz"):
        t = exchange(t.reshape(nz, 8, 2 * cols // 8), "z")
    low = t.astype(jnp.float32).sum(axis=0)
    low_value = low[:4].reshape(1, cols)
    low_output = low[4:].reshape(1, cols)

    next_first_value = 0.9 * first_value + 0.1 * low_value
    next_second_value = 0.95 * second_value + 0.05 * low_value * low_value
    next_first_output = 0.9 * first_output + 0.1 * low_output
    next_second_output = 0.95 * second_output + 0.05 * low_output * low_output
    direction_value = (next_first_value * lax.rsqrt(next_second_value)).astype(jnp.bfloat16)
    direction_output = (next_first_output * lax.rsqrt(next_second_output)).astype(jnp.bfloat16)
    d = jnp.concatenate([direction_value.reshape(4, -1), direction_output.reshape(4, -1)], axis=0)
    with jax.named_scope("dz"):
        d = to_all(d, "z")
    with jax.named_scope("dxc"):
        d = to_all(d, ("x", "c"))
    d = d.reshape(R, 2 * cols)
    d_value, d_output = d[:, :cols], d[:, cols:]

    update_value = jnp.dot(whole_value, d_value, preferred_element_type=jnp.float32)
    update_output = lax.dot_general(
        d_output, whole_output, (((0,), (1,)), ((), ())), preferred_element_type=jnp.float32
    )
    squares = jnp.stack([jnp.sum(update_value * update_value), jnp.sum(update_output * update_output)])
    with jax.named_scope("tot"):
        totals = to_all(jnp.broadcast_to(squares[:, None, None], (2, 8, 128)), "tp").sum(axis=0)
    entries = D * WIDTH
    scale_value = lax.rsqrt(totals[0, 0, 0] / entries + 1e-06)
    scale_output = lax.rsqrt(totals[1, 0, 0] / entries + 1e-06)

    at = lax.axis_index(FS) * rows
    own_value = jnp.dot(factor_value, jnp.dot(turn, d_value, preferred_element_type=jnp.float32).astype(jnp.bfloat16), preferred_element_type=jnp.float32)
    own_output = lax.dot_general(
        jnp.dot(turn, d_output, preferred_element_type=jnp.float32).astype(jnp.bfloat16), factor_output, (((0,), (1,)), ((), ())), preferred_element_type=jnp.float32
    )
    step_value = own_value * scale_value
    step_output = own_output * scale_output
    next_weight_value = weight_value - 0.02 * step_value
    next_weight_output = weight_output - 0.02 * step_output
    copy_value = (w[:, :cols] - (0.02 * scale_value) * update_value).astype(jnp.bfloat16)
    copy_output = (w[:, cols:].T - (0.02 * scale_output) * update_output).astype(jnp.bfloat16)
    return (
        step_value,
        step_output,
        next_weight_value,
        next_weight_output,
        next_first_value,
        next_second_value,
        next_first_output,
        next_second_output,
        copy_value,
        copy_output,
    )


def solution(mesh):
    torus = Mesh(mesh.devices.reshape(32, 4, 2, mesh.shape["tp"]), ("z", "x", "c", "tp"))
    placed = (
        P(FS, None),
        P(FS, "tp"),
        P(FS, "tp"),
        P(FS, None),
        P(FS, None),
        P(FS, None),
        P(FS, "tp"),
        P("tp", FS),
        P(FS, "tp"),
        P(FS, "tp"),
        P(FS, "tp"),
        P(FS, "tp"),
    )
    return jax.shard_map(
        body,
        mesh=torus,
        in_specs=placed,
        out_specs=(
            P(FS, "tp"),
            P("tp", FS),
            P(FS, "tp"),
            P("tp", FS),
            P(FS, "tp"),
            P(FS, "tp"),
            P(FS, "tp"),
            P(FS, "tp"),
            P(None, "tp"),
            P("tp", None),
        ),
        check_vma=False,
    )
```

```python
import jax
import jax.numpy as jnp
from jax import lax
from jax.experimental import pallas as pl
from jax.experimental.pallas import tpu as pltpu
from jax.sharding import Mesh
from jax.sharding import PartitionSpec as P

D = 2048
WIDTH = 2048
R = 256
FS = ("zh", "zl", "x", "c")
Z = ("zh", "zl")
LANES = 128
NT = (((1,), (1,)), ((), ()))
TN = (((0,), (0,)), ((), ()))


VMEM = pl.BlockSpec(memory_space=pltpu.VMEM)
SMEM = pl.BlockSpec(memory_space=pltpu.SMEM)
HBM = pl.BlockSpec(memory_space=pltpu.HBM)


def far(*arrays):
    return [pltpu.with_memory_space_constraint(a, pltpu.HBM) for a in arrays]


def params(mib):
    return pltpu.CompilerParams(vmem_limit_bytes=mib << 20)


def cost(flops, bytes_accessed):
    return pl.CostEstimate(flops=flops, bytes_accessed=bytes_accessed, transcendentals=0)


def dot(a, b, dims=(((1,), (0,)), ((), ()))):
    return lax.dot_general(a, b, dims, preferred_element_type=jnp.float32)


def eye(n):
    i = lax.broadcasted_iota(jnp.int32, (n, n), 0)
    return (i == lax.broadcasted_iota(jnp.int32, (n, n), 1)).astype(jnp.bfloat16)


def exchange(blocks, axes):
    return lax.all_to_all(blocks, axes, split_axis=0, concat_axis=0, tiled=True)


def to_all(block, axes):
    copies = jnp.broadcast_to(block[None], (lax.axis_size(axes), *block.shape))
    return exchange(copies, axes)


def moved(block, axis, by):
    n = lax.axis_size(axis)
    return lax.ppermute(block, axis, [(i, (i + by) % n) for i in range(n)])


def swapped(block, axis, bit):
    return lax.ppermute(block, axis, [(i, i ^ bit) for i in range(lax.axis_size(axis))])


def pack_kernel(place, fv, fo, wv, wo, out, fv_in, fo_in, wv_in, wo_in, sems):
    copies = [
        pltpu.make_async_copy(src, dst, sems.at[i])
        for i, (src, dst) in enumerate(((fv, fv_in), (fo, fo_in), (wv, wv_in), (wo, wo_in)))
    ]
    for copy in copies:
        copy.start()
    n = R // 8
    y = place[0]
    j = lax.broadcasted_iota(jnp.int32, (R, R), 0)
    k = lax.broadcasted_iota(jnp.int32, (R, R), 1)
    turn = (j == (k % n) * 8 + k // n).astype(jnp.bfloat16)
    for copy in copies:
        copy.wait()
    factor = jnp.where(y < 2, fv_in[...].astype(jnp.float32), fo_in[...].astype(jnp.float32))
    factor = dot(factor.astype(jnp.bfloat16), turn)
    tile = jnp.where(y % 2 == 0, factor[:, :LANES], factor[:, LANES:]).astype(jnp.bfloat16)
    tiles = [tile]
    for w in (wv_in, wo_in):
        half = w[...].astype(jnp.bfloat16)
        tiles += [half[:, t : t + LANES] for t in range(0, half.shape[1], LANES)]
    for t, tile in enumerate(tiles):
        out[:, t] = jnp.broadcast_to(tile[None], (out.shape[0], *tile.shape))


def packed(count, place, fv, fo, wv, wo):
    rows, cols = wv.shape
    tiles = 1 + 2 * cols // LANES
    return pl.pallas_call(
        pack_kernel,
        out_shape=jax.ShapeDtypeStruct((count, tiles, rows, LANES), jnp.bfloat16),
        in_specs=[SMEM, HBM, HBM, HBM, HBM],
        out_specs=VMEM,
        scratch_shapes=[
            pltpu.VMEM(fv.shape, fv.dtype),
            pltpu.VMEM(fo.shape, fo.dtype),
            pltpu.VMEM(wv.shape, wv.dtype),
            pltpu.VMEM(wo.shape, wo.dtype),
            pltpu.SemaphoreType.DMA((4,)),
        ],
        name="packed",
        compiler_params=params(4),
        cost_estimate=cost(2 * 8 * R * R, 200_000),
    )(place, *far(fv, fo, wv, wo))


def project_kernel(
    place, mine, other, xv, vv, xo, vo, out, fv, fo, whole, x_in, v_in, sems
):
    c = place[2]
    reads = [
        pltpu.make_async_copy(src, dst.at[f], sems.at[2 * f + k])
        for f, pair in enumerate(((xv, vv), (xo, vo)))
        for k, (src, dst) in enumerate(zip(pair, (x_in, v_in)))
    ]
    for copy in reads:
        copy.start()
    nzl, nx = whole.shape[2:4]
    half = R // LANES
    writes = []
    for f, target in enumerate((fv, fo)):
        for src, at in ((mine, c), (other, 1 - c)):
            for x in range(nx):
                for h in range(half):
                    for zl in range(nzl):
                        whole[f, :, zl, x, at, :, h * LANES : (h + 1) * LANES] = src[
                            x * 2 * half + f * half + h, zl
                        ]
        writes.append(pltpu.make_async_copy(whole.at[f], target, sems.at[4 + f]))
        writes[f].start()
    cols = vv.shape[1]
    for f in range(2):
        reads[2 * f].wait()
        projected = dot(x_in[f], whole[f].reshape(D, R)).astype(jnp.bfloat16)
        reads[2 * f + 1].wait()
        term = dot(projected, v_in[f], TN).astype(jnp.bfloat16)
        out[:, :, f * cols : (f + 1) * cols] = term.reshape(out.shape[0], out.shape[1], cols)
    for copy in writes:
        copy.wait()


def projected_terms(place, mine, other, xv, vv, xo, vo, sizes):
    nzh, nzl, nx, nc = sizes
    shape = (nzh, nzl, nx, nc, D // (nzh * nzl * nx * nc), R)
    whole = pltpu.HBM(shape, jnp.bfloat16)
    cols = vv.shape[1]
    tokens = xv.shape[0]
    return pl.pallas_call(
        project_kernel,
        out_shape=(
            jax.ShapeDtypeStruct((nx * nc, nzh * nzl, 2 * cols), jnp.bfloat16),
            whole,
            whole,
        ),
        in_specs=[SMEM, VMEM, VMEM, HBM, HBM, HBM, HBM],
        out_specs=(VMEM, HBM, HBM),
        scratch_shapes=[
            pltpu.VMEM((2, *shape), jnp.bfloat16),
            pltpu.VMEM((2, *xv.shape), jnp.bfloat16),
            pltpu.VMEM((2, *vv.shape), jnp.bfloat16),
            pltpu.SemaphoreType.DMA((6,)),
        ],
        name="project",
        compiler_params=params(20),
        cost_estimate=cost(4 * tokens * R * (D + cols), 10_000_000),
    )(place, mine, other, *far(xv, vv, xo, vo))


def summed_kernel(t, out, lines):
    total = jnp.sum(t[...].astype(jnp.float32), axis=0)
    nz, tiles, _ = out.shape
    for k in range(tiles):
        lines[pl.ds(k, nz, stride=tiles), :] = total[:, k * LANES : (k + 1) * LANES]
    out[...] = lines[...].reshape(out.shape).astype(jnp.bfloat16)


def summed(t):
    _, nz, width = t.shape
    tiles = width // LANES
    return pl.pallas_call(
        summed_kernel,
        out_shape=jax.ShapeDtypeStruct((nz, tiles, LANES), jnp.bfloat16),
        in_specs=[VMEM],
        out_specs=VMEM,
        scratch_shapes=[pltpu.VMEM((nz * tiles, LANES), jnp.float32)],
        name="summed",
        compiler_params=params(2),
        cost_estimate=cost(t.size, 600_000),
    )(t)


def gram_kernel(fv, fo, out, factors, grams, sems):
    reads = [
        pltpu.make_async_copy(src, factors.at[f], sems.at[f]) for f, src in enumerate((fv, fo))
    ]
    for copy in reads:
        copy.start()
    for f, copy in enumerate(reads):
        copy.wait()
        factor = factors[f].reshape(D, R)
        gram = dot(factor, factor, TN)
        high = gram.astype(jnp.bfloat16)
        grams[f, 0] = high
        grams[f, 1] = (gram - high.astype(jnp.float32)).astype(jnp.bfloat16)
    write = pltpu.make_async_copy(grams, out, sems.at[2])
    write.start()
    write.wait()


def gram_of(fv, fo):
    shape = (2, 2, R, R)
    return pl.pallas_call(
        gram_kernel,
        out_shape=pltpu.HBM(shape, jnp.bfloat16),
        in_specs=[HBM, HBM],
        out_specs=HBM,
        scratch_shapes=[
            pltpu.VMEM((2, *fv.shape), jnp.bfloat16),
            pltpu.VMEM(shape, jnp.bfloat16),
            pltpu.SemaphoreType.DMA((3,)),
        ],
        name="gram",
        compiler_params=params(8),
        cost_estimate=cost(4 * D * R * R, 3_000_000),
    )(*far(fv, fo))


def moments_kernel(t, fv, sv, fo, so, out, nfv, nsv, nfo, nso):
    low = jnp.sum(t[...].astype(jnp.float32), axis=0)
    half = low.shape[0] // 2
    directions = []
    for part, first, second, next_first, next_second in (
        (low[:half], fv, sv, nfv, nsv),
        (low[half:], fo, so, nfo, nso),
    ):
        a = 0.9 * first[...] + 0.1 * part
        b = 0.95 * second[...] + 0.05 * part * part
        next_first[...] = a
        next_second[...] = b
        directions.append(a * lax.rsqrt(b))
    d = jnp.concatenate(directions, axis=0).astype(jnp.bfloat16)
    out[...] = jnp.broadcast_to(d[None], out.shape)


def moments(t, *state):
    shape = jax.ShapeDtypeStruct(state[0].shape, jnp.float32)
    return pl.pallas_call(
        moments_kernel,
        out_shape=(jax.ShapeDtypeStruct(t.shape, jnp.bfloat16), shape, shape, shape, shape),
        in_specs=[VMEM] * 5,
        out_specs=(VMEM,) * 5,
        name="moments",
        compiler_params=params(2),
        cost_estimate=cost(100_000, 150_000),
    )(t, *state)


def total_kernel(d, gram, out, dv, turned, gram_in, lines, whole, across, sems):
    read = pltpu.make_async_copy(gram, gram_in, sems.at[0])
    read.start()
    tiles = d.shape[1]
    lines[...] = d[...].astype(jnp.float32).reshape(lines.shape)
    for k in range(tiles):
        part = lines[pl.ds(k, R, stride=tiles), :].astype(jnp.bfloat16)
        whole[k // (tiles // 2), :, pl.ds(k % (tiles // 2) * LANES, LANES)] = part
    write_v = pltpu.make_async_copy(whole.at[0], dv, sems.at[1])
    write_v.start()
    across[...] = dot(eye(across.shape[0]), whole[1], NT).astype(jnp.bfloat16)
    write_o = pltpu.make_async_copy(across, turned, sems.at[2])
    write_o.start()
    read.wait()
    rows = out.shape[1] // 2
    for f in range(2):
        part = whole[f]
        square = part.astype(jnp.float32) * (dot(gram_in[f, 0], part) + dot(gram_in[f, 1], part))
        out[:, f * rows : (f + 1) * rows] = jnp.full(
            (out.shape[0], rows, LANES), jnp.sum(square)
        )
    write_v.wait()
    write_o.wait()


def totals_of(count, d, gram):
    _, tiles, _ = d.shape
    cols = tiles // 2 * LANES
    return pl.pallas_call(
        total_kernel,
        out_shape=(
            jax.ShapeDtypeStruct((count, 8, LANES), jnp.float32),
            pltpu.HBM((R, cols), jnp.bfloat16),
            pltpu.HBM((cols, R), jnp.bfloat16),
        ),
        in_specs=[VMEM, HBM],
        out_specs=(VMEM, HBM, HBM),
        scratch_shapes=[
            pltpu.VMEM(gram.shape, jnp.bfloat16),
            pltpu.VMEM((R * tiles, LANES), jnp.float32),
            pltpu.VMEM((2, R, cols), jnp.bfloat16),
            pltpu.VMEM((cols, R), jnp.bfloat16),
            pltpu.SemaphoreType.DMA((3,)),
        ],
        name="totals",
        compiler_params=params(6),
        cost_estimate=cost(8 * R * R * cols, 2_000_000),
    )(d, *far(gram))


def assemble_kernel(place, *refs):
    parts, (value, output, tiles_in, turned, sems) = refs[:-5], refs[-5:]
    zl, x, c = place[1], place[3], place[2]
    nx = len(parts) // 2
    nzl, nzh = parts[0].shape[:2]
    half = (parts[0].shape[2] - 1) // 2
    reads = []
    for f in range(2):
        for k, part in enumerate(parts):
            px = lax.rem(x + nx - k % nx, nx)
            pc = c if k < nx else 1 - c
            for s in range(nzl):
                reads.append(
                    pltpu.make_async_copy(
                        part.at[s, :, pl.ds(1 + f * half, half)],
                        tiles_in.at[f, :, lax.bitwise_xor(zl, s), px, pc],
                        sems.at[f],
                    )
                )
    for copy in reads:
        copy.start()
    for copy in reads[: len(reads) // 2]:
        copy.wait()
    write_v = pltpu.make_async_copy(tiles_in.at[0], value, sems.at[2])
    write_v.start()
    for copy in reads[len(reads) // 2 :]:
        copy.wait()
    chunk = D // nzh
    one = eye(half * LANES)
    for i in range(nzh):
        w = tiles_in[1, i]
        w = jnp.concatenate(
            [w[:, :, :, t].reshape(chunk, LANES) for t in range(half)], axis=1
        )
        turned[:, i * chunk : (i + 1) * chunk] = dot(one, w, NT).astype(jnp.bfloat16)
    write_o = pltpu.make_async_copy(turned, output, sems.at[3])
    write_o.start()
    write_v.wait()
    write_o.wait()


def assembled(place, parts, sizes):
    nzh, nzl, nx, nc = sizes
    _, _, tiles, rows, _ = parts[0].shape
    half = (tiles - 1) // 2
    cols = half * LANES
    shape = (nzh, nzl, nx, nc, half, rows, LANES)
    value, output = pl.pallas_call(
        assemble_kernel,
        out_shape=(
            pltpu.HBM(shape, jnp.bfloat16),
            pltpu.HBM((cols, D), jnp.bfloat16),
        ),
        in_specs=[SMEM] + [HBM] * len(parts),
        out_specs=(HBM, HBM),
        scratch_shapes=[
            pltpu.VMEM((2, *shape), jnp.bfloat16),
            pltpu.VMEM((cols, D), jnp.bfloat16),
            pltpu.SemaphoreType.DMA((4,)),
        ],
        name="assemble",
        compiler_params=params(12),
        cost_estimate=cost(2 * cols * cols * D, 9_000_000),
    )(place, *far(*parts))
    return value.reshape(D // rows, half, rows, LANES), output


def final_kernel(place, totals, dv, turned, fv, fo, wv, wo, ov, oo, own_v, own_o, copy_v, copy_o, sv, so, nv, no):
    entries = D * WIDTH
    sums = jnp.sum(totals[...], axis=0)
    scale = lax.rsqrt(sums / entries + 1e-06)
    scale_v, scale_o = scale[:1, :1], scale[4:5, :1]
    chunk = copy_v.shape[0]

    @pl.when(pl.program_id(0) == 0)
    def _():
        step_v = dot(own_v[0], dv[...]) * scale_v
        step_o = dot(own_o[0], turned[...], NT) * scale_o
        sv[...] = step_v
        so[...] = step_o
        nv[...] = ov[...] - 0.02 * step_v
        no[...] = oo[...] - 0.02 * step_o

    whole_v = fv[...].reshape(chunk, R)
    whole_o = fo[...].reshape(chunk, R)
    update = dot(whole_v, dv[...]) * (0.02 * scale_v)
    for t in range(wv.shape[1]):
        lanes = slice(t * LANES, (t + 1) * LANES)
        copy_v[:, lanes] = (
            wv[:, t].astype(jnp.float32).reshape(chunk, LANES) - update[:, lanes]
        ).astype(jnp.bfloat16)
    copy_o[...] = (
        wo[...].astype(jnp.float32) - dot(turned[...], whole_o, NT) * (0.02 * scale_o)
    ).astype(jnp.bfloat16)


def final(place, totals, dv, turned, fv, fo, wv, wo, ov, oo):
    cols = turned.shape[0]
    rows = ov.shape[0]
    steps = 8
    chunk = D // steps
    own = pltpu.HBM(ov.shape, jnp.float32)
    factor = pl.BlockSpec((chunk // rows, rows, R), lambda i, p: (i, 0, 0))
    mine = pl.BlockSpec((1, rows, R), lambda i, p: (p[4], 0, 0))
    down = pl.BlockSpec((chunk, cols), lambda i, p: (i, 0))
    across = pl.BlockSpec((cols, chunk), lambda i, p: (0, i))
    blocks = pl.BlockSpec((chunk // rows, wv.shape[1], rows, LANES), lambda i, p: (i, 0, 0, 0))

    def same(a):
        return pl.BlockSpec(a.shape, lambda i, p: (0,) * a.ndim)

    return pl.pallas_call(
        final_kernel,
        out_shape=(
            pltpu.HBM((D, cols), jnp.bfloat16),
            pltpu.HBM((cols, D), jnp.bfloat16),
            own,
            own,
            own,
            own,
        ),
        grid_spec=pltpu.PrefetchScalarGridSpec(
            num_scalar_prefetch=1,
            grid=(steps,),
            in_specs=[same(totals), same(dv), same(turned), factor, factor, blocks, across]
            + [same(ov), same(oo), mine, mine],
            out_specs=(down, across, same(ov), same(ov), same(ov), same(ov)),
        ),
        name="final",
        compiler_params=params(60),
        cost_estimate=cost(4 * D * cols * R, 10_000_000),
    )(place, totals, *far(dv, turned, fv, fo, wv, wo, ov, oo, fv, fo))


def step(
    normed_input,
    value_cotangent,
    gated_output,
    layer_cotangent,
    factor_value,
    factor_output,
    weight_value,
    weight_output,
    first_value,
    second_value,
    first_output,
    second_output,
):
    sizes = tuple(lax.axis_size(a) for a in FS)
    nzh, _, _, _ = sizes
    ny = lax.axis_size("tp")
    rows, cols = weight_value.shape

    at = [lax.axis_index(a) for a in ("tp", "zl", "c", "x", FS)]
    place = jnp.stack(at).astype(jnp.int32)
    turned_weight = weight_output.T
    w = exchange(packed(nzh, place, factor_value, factor_output, weight_value, turned_weight), "zh")
    f = to_all(w[:, 0], "zl")
    f = to_all(f, ("x", "tp"))
    other = moved(f, "c", 1)

    wa = swapped(w, "zl", 1)
    wa = jnp.stack([w, wa])
    wb = swapped(wa, "zl", 2)
    w0 = jnp.concatenate([wa, wb])

    terms, whole_value, whole_output = projected_terms(
        place, f, other, normed_input, value_cotangent, layer_cotangent, gated_output, sizes
    )
    t = exchange(terms, ("x", "c"))
    t = summed(t)
    t = exchange(t, Z)

    w1 = moved(w0, "x", 1)
    w3 = moved(w0, "x", 3)
    v0 = moved(w0, "c", 1)

    narrow = (2 * cols // (8 * LANES) * 4, LANES)
    d, *state = moments(
        t, *(s.reshape(narrow) for s in (first_value, second_value, first_output, second_output))
    )
    next_first_value, next_second_value, next_first_output, next_second_output = (
        s.reshape(1, cols) for s in state
    )
    d = exchange(d, Z)

    w2 = moved(w1, "x", 1)
    v1 = moved(w1, "c", 1)
    v3 = moved(w3, "c", 1)

    d = to_all(d, ("x", "c"))
    v2 = moved(w2, "c", 1)
    totals, dv, turned = totals_of(
        ny, d.reshape(R, *d.shape[2:]), gram_of(whole_value, whole_output)
    )
    totals = exchange(totals, "tp")

    all_value, all_output = assembled(place, (w0, w1, w2, w3, v0, v1, v2, v3), sizes)
    blocks = (D // rows, rows, R)
    copy_value, copy_output, step_value, step_output, next_value, next_output = final(
        place,
        totals,
        dv,
        turned,
        whole_value.reshape(blocks),
        whole_output.reshape(blocks),
        all_value,
        all_output,
        weight_value,
        turned_weight,
    )
    return (
        step_value,
        step_output.T,
        next_value,
        next_output.T,
        next_first_value,
        next_second_value,
        next_first_output,
        next_second_output,
        copy_value,
        copy_output,
    )


def solution(mesh):
    torus = Mesh(
        mesh.devices.reshape(8, 4, 4, 2, mesh.shape["tp"]), ("zh", "zl", "x", "c", "tp")
    )
    placed = (
        P(FS, None),
        P(FS, "tp"),
        P(FS, "tp"),
        P(FS, None),
        P(FS, None),
        P(FS, None),
        P(FS, "tp"),
        P("tp", FS),
        P(FS, "tp"),
        P(FS, "tp"),
        P(FS, "tp"),
        P(FS, "tp"),
    )
    return jax.shard_map(
        step,
        mesh=torus,
        in_specs=placed,
        out_specs=(
            P(FS, "tp"),
            P("tp", FS),
            P(FS, "tp"),
            P("tp", FS),
            P(FS, "tp"),
            P(FS, "tp"),
            P(FS, "tp"),
            P(FS, "tp"),
            P(None, "tp"),
            P("tp", None),
        ),
        check_vma=False,
    )
```

```python
import jax
import jax.numpy as jnp
from jax import lax
from jax.experimental import pallas as pl
from jax.experimental.pallas import tpu as pltpu
from jax.sharding import Mesh
from jax.sharding import PartitionSpec as P

D = 2048
WIDTH = 2048
R = 256
FS = ("zh", "zl", "x", "c")
Z = ("zh", "zl")
LANES = 128
TN = (((0,), (0,)), ((), ()))


VMEM = pl.BlockSpec(memory_space=pltpu.VMEM)
SMEM = pl.BlockSpec(memory_space=pltpu.SMEM)
HBM = pl.BlockSpec(memory_space=pltpu.HBM)


def far(*arrays):
    return [pltpu.with_memory_space_constraint(a, pltpu.HBM) for a in arrays]


def near(*arrays):
    return [pltpu.with_memory_space_constraint(a, pltpu.VMEM) for a in arrays]


def params(mib):
    return pltpu.CompilerParams(vmem_limit_bytes=mib << 20)


def cost(flops, bytes_accessed):
    return pl.CostEstimate(flops=flops, bytes_accessed=bytes_accessed, transcendentals=0)


def dot(a, b, dims=(((1,), (0,)), ((), ()))):
    return lax.dot_general(a, b, dims, preferred_element_type=jnp.float32)


def exchange(blocks, axes):
    return lax.all_to_all(blocks, axes, split_axis=0, concat_axis=0, tiled=True)


def to_all(block, axes):
    copies = jnp.broadcast_to(block[None], (lax.axis_size(axes), *block.shape))
    return exchange(copies, axes)


def moved(block, axis, by):
    n = lax.axis_size(axis)
    return lax.ppermute(block, axis, [(i, (i + by) % n) for i in range(n)])


def swapped(block, axis, bit):
    return lax.ppermute(block, axis, [(i, i ^ bit) for i in range(lax.axis_size(axis))])


def pack_kernel(place, fv, fo, wv, wo, vv, vo, out, vv_in, vo_in, fv_in, fo_in, wv_in, wo_in, sems):
    copies = [
        pltpu.make_async_copy(src, dst, sems.at[i])
        for i, (src, dst) in enumerate(
            ((fv, fv_in), (fo, fo_in), (wv, wv_in), (wo, wo_in), (vv, vv_in), (vo, vo_in))
        )
    ]
    for copy in copies:
        copy.start()
    n = R // 8
    y = place[0]
    j = lax.broadcasted_iota(jnp.int32, (R, R), 0)
    k = lax.broadcasted_iota(jnp.int32, (R, R), 1)
    turn = (j == (k % n) * 8 + k // n).astype(jnp.bfloat16)
    for copy in copies[:4]:
        copy.wait()
    factor = jnp.where(y < 2, fv_in[...].astype(jnp.float32), fo_in[...].astype(jnp.float32))
    factor = dot(factor.astype(jnp.bfloat16), turn)
    tile = jnp.where(y % 2 == 0, factor[:, :LANES], factor[:, LANES:]).astype(jnp.bfloat16)
    tiles = [tile]
    for w in (wv_in, wo_in):
        half = w[...].astype(jnp.bfloat16)
        tiles += [half[:, t : t + LANES] for t in range(0, half.shape[1], LANES)]
    for t, tile in enumerate(tiles):
        out[:, t] = jnp.broadcast_to(tile[None], (out.shape[0], *tile.shape))
    for copy in copies[4:]:
        copy.wait()


def packed(count, place, fv, fo, wv, wo, vv, vo):
    rows, cols = wv.shape
    tiles = 1 + 2 * cols // LANES
    return pl.pallas_call(
        pack_kernel,
        out_shape=(
            jax.ShapeDtypeStruct((count, tiles, rows, LANES), jnp.bfloat16),
            pltpu.VMEM(vv.shape, vv.dtype),
            pltpu.VMEM(vo.shape, vo.dtype),
        ),
        in_specs=[SMEM] + [HBM] * 6,
        out_specs=(VMEM,) * 3,
        scratch_shapes=[
            pltpu.VMEM(fv.shape, fv.dtype),
            pltpu.VMEM(fo.shape, fo.dtype),
            pltpu.VMEM(wv.shape, wv.dtype),
            pltpu.VMEM(wo.shape, wo.dtype),
            pltpu.SemaphoreType.DMA((6,)),
        ],
        name="packed",
        compiler_params=params(4),
        cost_estimate=cost(2 * 8 * R * R, 200_000),
    )(place, *far(fv, fo, wv, wo, vv, vo))


def project_kernel(place, mine, other, xv, vv, xo, vo, out, whole):
    c = place[2]
    nzl, nx = whole.shape[2:4]
    half = R // LANES
    cols = vv.shape[1]
    for f in range(2):
        for src, at in ((mine, c), (other, 1 - c)):
            for x in range(nx):
                for h in range(half):
                    for zl in range(nzl):
                        whole[f, :, zl, x, at, :, h * LANES : (h + 1) * LANES] = src[
                            x * 2 * half + f * half + h, zl
                        ]
    for f, (x, v) in enumerate(((xv, vv), (xo, vo))):
        projected = dot(x[...], whole[f].reshape(D, R)).astype(jnp.bfloat16)
        term = dot(projected, v[...], TN).astype(jnp.bfloat16)
        out[:, :, f * cols : (f + 1) * cols] = term.reshape(out.shape[0], out.shape[1], cols)


def projected_terms(place, mine, other, xv, vv, xo, vo, sizes):
    nzh, nzl, nx, nc = sizes
    shape = (2, nzh, nzl, nx, nc, D // (nzh * nzl * nx * nc), R)
    cols = vv.shape[1]
    tokens = xv.shape[0]
    return pl.pallas_call(
        project_kernel,
        out_shape=(
            jax.ShapeDtypeStruct((nx * nc, nzh * nzl, 2 * cols), jnp.bfloat16),
            pltpu.VMEM(shape, jnp.bfloat16),
        ),
        in_specs=[SMEM] + [VMEM] * 6,
        out_specs=(VMEM, VMEM),
        name="project",
        compiler_params=params(12),
        cost_estimate=cost(4 * tokens * R * (D + cols), 10_000_000),
    )(place, mine, other, *near(xv, vv, xo, vo))


def summed_kernel(t, out, lines):
    total = jnp.sum(t[...].astype(jnp.float32), axis=0)
    nz, tiles, _ = out.shape
    for k in range(tiles):
        lines[pl.ds(k, nz, stride=tiles), :] = total[:, k * LANES : (k + 1) * LANES]
    out[...] = lines[...].reshape(out.shape).astype(jnp.bfloat16)


def summed(t):
    _, nz, width = t.shape
    tiles = width // LANES
    return pl.pallas_call(
        summed_kernel,
        out_shape=jax.ShapeDtypeStruct((nz, tiles, LANES), jnp.bfloat16),
        in_specs=[VMEM],
        out_specs=VMEM,
        scratch_shapes=[pltpu.VMEM((nz * tiles, LANES), jnp.float32)],
        name="summed",
        compiler_params=params(2),
        cost_estimate=cost(t.size, 600_000),
    )(t)


def gram_kernel(factors, grams):
    for f in range(2):
        factor = factors[f].reshape(D, R)
        gram = dot(factor, factor, TN)
        high = gram.astype(jnp.bfloat16)
        grams[f, 0] = high
        grams[f, 1] = (gram - high.astype(jnp.float32)).astype(jnp.bfloat16)


def gram_of(factors):
    shape = (2, 2, R, R)
    return pl.pallas_call(
        gram_kernel,
        out_shape=pltpu.VMEM(shape, jnp.bfloat16),
        in_specs=[VMEM],
        out_specs=VMEM,
        name="gram",
        compiler_params=params(8),
        cost_estimate=cost(4 * D * R * R, 3_000_000),
    )(*near(factors))


def moments_kernel(t, fv, sv, fo, so, out, nfv, nsv, nfo, nso):
    low = jnp.sum(t[...].astype(jnp.float32), axis=0)
    half = low.shape[0] // 2
    directions = []
    for part, first, second, next_first, next_second in (
        (low[:half], fv, sv, nfv, nsv),
        (low[half:], fo, so, nfo, nso),
    ):
        a = 0.9 * first[...] + 0.1 * part
        b = 0.95 * second[...] + 0.05 * part * part
        next_first[...] = a
        next_second[...] = b
        directions.append(a * lax.rsqrt(b))
    d = jnp.concatenate(directions, axis=0).astype(jnp.bfloat16)
    out[...] = jnp.broadcast_to(d[None], out.shape)


def moments(t, *state):
    shape = jax.ShapeDtypeStruct(state[0].shape, jnp.float32)
    return pl.pallas_call(
        moments_kernel,
        out_shape=(jax.ShapeDtypeStruct(t.shape, jnp.bfloat16), shape, shape, shape, shape),
        in_specs=[VMEM] * 5,
        out_specs=(VMEM,) * 5,
        name="moments",
        compiler_params=params(2),
        cost_estimate=cost(100_000, 150_000),
    )(t, *state)


def total_kernel(d, gram, out, whole, lines):
    tiles = d.shape[1]
    half = tiles // 2
    lines[...] = d[...].astype(jnp.float32).reshape(lines.shape)
    parts = [lines[pl.ds(k, R, stride=tiles), :].astype(jnp.bfloat16) for k in range(tiles)]
    rows = out.shape[1] // 2
    for f in range(2):
        part = jnp.concatenate(parts[f * half : (f + 1) * half], axis=1)
        whole[f] = part
        square = part.astype(jnp.float32) * (dot(gram[f, 0], part) + dot(gram[f, 1], part))
        out[:, f * rows : (f + 1) * rows] = jnp.full(
            (out.shape[0], rows, LANES), jnp.sum(square)
        )


def totals_of(count, d, gram):
    _, tiles, _ = d.shape
    cols = tiles // 2 * LANES
    return pl.pallas_call(
        total_kernel,
        out_shape=(
            jax.ShapeDtypeStruct((count, 8, LANES), jnp.float32),
            pltpu.VMEM((2, R, cols), jnp.bfloat16),
        ),
        in_specs=[VMEM, VMEM],
        out_specs=(VMEM, VMEM),
        scratch_shapes=[pltpu.VMEM((R * tiles, LANES), jnp.float32)],
        name="totals",
        compiler_params=params(6),
        cost_estimate=cost(8 * R * R * cols, 2_000_000),
    )(d, *near(gram))


def assemble_kernel(place, *refs):
    parts, out = refs[:-2], refs[-1]
    zl, x = place[1], place[3]
    nx = len(parts)
    for k, part in enumerate(parts):
        px = lax.rem(x + nx - k, nx)
        for s in range(part.shape[0]):
            for t in range(part.shape[2] - 1):
                lanes = slice(t * LANES, (t + 1) * LANES)
                out[:, lax.bitwise_xor(zl, s), px, :, lanes] = part[s, :, 1 + t]


def assembled(place, parts, sizes, after):
    nzh, nzl, nx, _ = sizes
    tiles, rows = parts[0].shape[2:4]
    shape = (nzh, nzl, nx, rows, (tiles - 1) * LANES)
    return pl.pallas_call(
        assemble_kernel,
        out_shape=jax.ShapeDtypeStruct(shape, jnp.bfloat16),
        in_specs=[SMEM] + [VMEM] * len(parts) + [pl.BlockSpec(memory_space=pl.ANY)],
        out_specs=VMEM,
        name="assemble",
        compiler_params=params(8),
        cost_estimate=cost(1_000_000, 4_000_000),
    )(place, *near(*parts), after)


def final_kernel(place, totals, directions, factors, mine, other, ov, oo, *refs):
    copy_v, copy_o, sv, so, nv, no, out_v, out_o, sems = refs
    steps, nzl, nx, nc, rows, _ = factors.shape[1:]
    chunk = D // steps
    cols = directions.shape[2]
    sums = jnp.sum(totals[...], axis=0)
    scale = lax.rsqrt(sums / (D * WIDTH) + 1e-06)
    scales = scale[:1, :1], scale[4:5, :1]
    writes = []
    for k in range(2):
        part = pl.ds(k * steps // 2, steps // 2)
        lanes = pl.ds(k * D // 2, D // 2)
        writes += [
            pltpu.make_async_copy(out_v.at[part], copy_v.at[part], sems.at[2 * k]),
            pltpu.make_async_copy(out_o.at[:, lanes], copy_o.at[:, lanes], sems.at[2 * k + 1]),
        ]

    def copies(pair):
        for i in range(steps):
            for c in range(nc):
                factor = factors[0, i, :, :, c].reshape(chunk // nc, R)
                update = dot(factor, directions[0]) * (0.02 * scales[0])
                w = pair[c][i, :, :, :, :cols].reshape(chunk // nc, cols).astype(jnp.float32)
                out_v[i, :, :, c] = (w - update).astype(jnp.bfloat16).reshape(nzl, nx, rows, cols)
            if (i + 1) * 2 % steps == 0:
                writes[(i + 1) * 4 // steps - 2].start()
            update = dot(factors[1, i].reshape(chunk, R), directions[1]) * (0.02 * scales[1])
            w = jnp.stack([p[i, :, :, :, cols:] for p in pair], axis=2).reshape(chunk, cols)
            half = (w.astype(jnp.float32) - update).astype(jnp.bfloat16)
            out_o[:, i * chunk : (i + 1) * chunk] = half.T
            if (i + 1) * 2 % steps == 0:
                writes[(i + 1) * 4 // steps - 1].start()

    first = place[2] == 0

    @pl.when(first)
    def _():
        copies((mine, other))

    @pl.when(jnp.logical_not(first))
    def _():
        copies((other, mine))

    for f, (w, step, after) in enumerate(((ov, sv, nv), (oo, so, no))):
        own = factors[f, place[5], place[1], place[3], place[2]]
        step[...] = dot(own, directions[f]) * scales[f]
        after[...] = w[...] - 0.02 * step[...]
    for copy in writes:
        copy.wait()


def final(place, totals, directions, factors, mine, other, ov, oo):
    cols = directions.shape[2]
    own = jax.ShapeDtypeStruct(ov.shape, jnp.float32)
    shape = (*factors.shape[1:-1], cols)
    copy_value, *rest = pl.pallas_call(
        final_kernel,
        out_shape=(
            pltpu.HBM(shape, jnp.bfloat16),
            pltpu.HBM((cols, D), jnp.bfloat16),
            own,
            own,
            own,
            own,
        ),
        in_specs=[SMEM] + [VMEM] * 7,
        out_specs=(HBM, HBM, VMEM, VMEM, VMEM, VMEM),
        scratch_shapes=[
            pltpu.VMEM(shape, jnp.bfloat16),
            pltpu.VMEM((cols, D), jnp.bfloat16),
            pltpu.SemaphoreType.DMA((4,)),
        ],
        name="final",
        compiler_params=params(12),
        cost_estimate=cost(4 * D * cols * R, 10_000_000),
    )(place, totals, *near(directions, factors, mine, other), ov, oo)
    return copy_value.reshape(D, cols), *rest


def step(
    normed_input,
    value_cotangent,
    gated_output,
    layer_cotangent,
    factor_value,
    factor_output,
    weight_value,
    weight_output,
    first_value,
    second_value,
    first_output,
    second_output,
):
    sizes = tuple(lax.axis_size(a) for a in FS)
    nzh, _, _, _ = sizes
    ny = lax.axis_size("tp")
    _, cols = weight_value.shape

    at = [lax.axis_index(a) for a in ("tp", "zl", "c", "x", FS, "zh")]
    place = jnp.stack(at).astype(jnp.int32)
    turned_weight = weight_output.T
    w, value_near, output_near = packed(
        nzh,
        place,
        factor_value,
        factor_output,
        weight_value,
        turned_weight,
        value_cotangent,
        gated_output,
    )
    w = exchange(w, "zh")
    f = to_all(w[:, 0], "zl")
    f = to_all(f, ("x", "tp"))
    other = moved(f, "c", 1)

    get = swapped(w, "zl", 1)
    w = jnp.stack([w, get])
    get = swapped(w, "zl", 2)
    w0 = jnp.concatenate([w, get])

    terms, factors = projected_terms(
        place, f, other, normed_input, value_near, layer_cotangent, output_near, sizes
    )
    t = exchange(terms, ("x", "c"))
    t = summed(t)
    t = exchange(t, Z)
    gram = gram_of(factors)

    w1 = moved(w0, "x", 1)
    w3 = moved(w0, "x", 3)

    narrow = (2 * cols // (8 * LANES) * 4, LANES)
    d, *state = moments(
        t, *(s.reshape(narrow) for s in (first_value, second_value, first_output, second_output))
    )
    next_first_value, next_second_value, next_first_output, next_second_output = (
        s.reshape(1, cols) for s in state
    )
    d = exchange(d, Z)

    w2 = moved(w1, "x", 1)
    d = to_all(d, ("x", "c"))
    mine = assembled(place, (w0, w1, w2, w3), sizes, d)
    flip = moved(mine, "c", 1)

    totals, directions = totals_of(ny, d.reshape(R, *d.shape[2:]), gram)
    totals = exchange(totals, "tp")

    copy_value, copy_output, step_value, step_output, next_value, next_output = final(
        place,
        totals,
        directions,
        factors,
        mine,
        flip,
        weight_value,
        turned_weight,
    )
    return (
        step_value,
        step_output.T,
        next_value,
        next_output.T,
        next_first_value,
        next_second_value,
        next_first_output,
        next_second_output,
        copy_value,
        copy_output,
    )


def solution(mesh):
    torus = Mesh(
        mesh.devices.reshape(8, 4, 4, 2, mesh.shape["tp"]), ("zh", "zl", "x", "c", "tp")
    )
    placed = (
        P(FS, None),
        P(FS, "tp"),
        P(FS, "tp"),
        P(FS, None),
        P(FS, None),
        P(FS, None),
        P(FS, "tp"),
        P("tp", FS),
        P(FS, "tp"),
        P(FS, "tp"),
        P(FS, "tp"),
        P(FS, "tp"),
    )
    return jax.shard_map(
        step,
        mesh=torus,
        in_specs=placed,
        out_specs=(
            P(FS, "tp"),
            P("tp", FS),
            P(FS, "tp"),
            P("tp", FS),
            P(FS, "tp"),
            P(FS, "tp"),
            P(FS, "tp"),
            P(FS, "tp"),
            P(None, "tp"),
            P("tp", None),
        ),
        check_vma=False,
    )
```

```python
import jax
import jax.numpy as jnp
from jax import lax
from jax.experimental import pallas as pl
from jax.experimental.pallas import tpu as pltpu
from jax.sharding import Mesh
from jax.sharding import PartitionSpec as P

D = 2048
WIDTH = 2048
R = 256
FS = ("z", "x", "c")
NZL = 4
LANES = 128
TN = (((0,), (0,)), ((), ()))


VMEM = pl.BlockSpec(memory_space=pltpu.VMEM)
SMEM = pl.BlockSpec(memory_space=pltpu.SMEM)
HBM = pl.BlockSpec(memory_space=pltpu.HBM)


def far(*arrays):
    return [pltpu.with_memory_space_constraint(a, pltpu.HBM) for a in arrays]


def near(*arrays):
    return [pltpu.with_memory_space_constraint(a, pltpu.VMEM) for a in arrays]


def params(mib):
    return pltpu.CompilerParams(vmem_limit_bytes=mib << 20)


def cost(flops, bytes_accessed):
    return pl.CostEstimate(flops=flops, bytes_accessed=bytes_accessed, transcendentals=0)


def dot(a, b, dims=(((1,), (0,)), ((), ()))):
    return lax.dot_general(a, b, dims, preferred_element_type=jnp.float32)


def turned(n, by):
    return [(i + by) % n for i in range(n)]


def near_z(nz):
    return [[i + k for k in (1, 0, 2, 3)] for i in range(0, nz, NZL)]


def far_z(nz):
    n = nz // NZL
    return [[i + NZL * k for k in turned(n, n // 2)] for i in range(NZL)]


def exchange(blocks, axes, groups=None):
    return lax.all_to_all(
        blocks, axes, split_axis=0, concat_axis=0, axis_index_groups=groups, tiled=True
    )


def to_all(block, axes, groups=None):
    count = len(groups[0]) if groups else lax.axis_size(axes)
    copies = jnp.broadcast_to(block[None], (count, *block.shape))
    return exchange(copies, axes, groups)


def moved(block, axis, by):
    n = lax.axis_size(axis)
    return lax.ppermute(block, axis, [(i, (i + by) % n) for i in range(n)])


def swapped(block, axis, bit):
    return lax.ppermute(block, axis, [(i, i ^ bit) for i in range(lax.axis_size(axis))])


def pack_kernel(place, fv, fo, wv, wo, vv, vo, out, vv_in, vo_in, fv_in, fo_in, wv_in, wo_in, sems):
    copies = [
        pltpu.make_async_copy(src, dst, sems.at[i])
        for i, (src, dst) in enumerate(
            ((fv, fv_in), (fo, fo_in), (wv, wv_in), (wo, wo_in), (vv, vv_in), (vo, vo_in))
        )
    ]
    for copy in copies:
        copy.start()
    n = R // 8
    y = place[0]
    j = lax.broadcasted_iota(jnp.int32, (R, R), 0)
    k = lax.broadcasted_iota(jnp.int32, (R, R), 1)
    turn = (j == (k % n + n // 2) % n * 8 + k // n).astype(jnp.bfloat16)
    for copy in copies[:4]:
        copy.wait()
    factor = jnp.where(y < 2, fv_in[...].astype(jnp.float32), fo_in[...].astype(jnp.float32))
    factor = dot(factor.astype(jnp.bfloat16), turn)
    tile = jnp.where(y % 2 == 0, factor[:, :LANES], factor[:, LANES:]).astype(jnp.bfloat16)
    tiles = [tile]
    for w in (wv_in, wo_in):
        half = w[...].astype(jnp.bfloat16)
        tiles += [half[:, t : t + LANES] for t in range(0, half.shape[1], LANES)]
    for t, tile in enumerate(tiles):
        out[:, t] = jnp.broadcast_to(tile[None], (out.shape[0], *tile.shape))
    for copy in copies[4:]:
        copy.wait()


def packed(count, place, fv, fo, wv, wo, vv, vo):
    rows, cols = wv.shape
    tiles = 1 + 2 * cols // LANES
    return pl.pallas_call(
        pack_kernel,
        out_shape=(
            jax.ShapeDtypeStruct((count, tiles, rows, LANES), jnp.bfloat16),
            pltpu.VMEM(vv.shape, vv.dtype),
            pltpu.VMEM(vo.shape, vo.dtype),
        ),
        in_specs=[SMEM] + [HBM] * 6,
        out_specs=(VMEM,) * 3,
        scratch_shapes=[
            pltpu.VMEM(fv.shape, fv.dtype),
            pltpu.VMEM(fo.shape, fo.dtype),
            pltpu.VMEM(wv.shape, wv.dtype),
            pltpu.VMEM(wo.shape, wo.dtype),
            pltpu.SemaphoreType.DMA((6,)),
        ],
        name="packed",
        compiler_params=params(4),
        cost_estimate=cost(2 * 8 * R * R, 200_000),
    )(place, *far(fv, fo, wv, wo, vv, vo))


def project_kernel(place, mine, other, xv, vv, xo, vo, out, whole):
    c = place[2]
    nzh, nzl, nx = whole.shape[1:4]
    first = nzh // 2
    half = R // LANES
    cols = vv.shape[1]
    for f in range(2):
        for src, at in ((mine, c), (other, 1 - c)):
            for x in range(nx):
                for h in range(half):
                    for k, zl in enumerate(near_z(nzl)[0]):
                        lanes = slice(h * LANES, (h + 1) * LANES)
                        block = src.at[x * 2 * half + f * half + h, k]
                        whole[f, first:, zl, x, at, :, lanes] = block[: nzh - first]
                        whole[f, :first, zl, x, at, :, lanes] = block[nzh - first :]
    for f, (x, v) in enumerate(((xv, vv), (xo, vo))):
        projected = dot(x[...], whole[f].reshape(D, R)).astype(jnp.bfloat16)
        term = dot(projected, v[...], TN).astype(jnp.bfloat16)
        out[:, :, f * cols : (f + 1) * cols] = term.reshape(out.shape[0], out.shape[1], cols)


def projected_terms(place, mine, other, xv, vv, xo, vo, sizes):
    nzh, nzl, nx, nc = sizes
    shape = (2, nzh, nzl, nx, nc, D // (nzh * nzl * nx * nc), R)
    cols = vv.shape[1]
    tokens = xv.shape[0]
    return pl.pallas_call(
        project_kernel,
        out_shape=(
            jax.ShapeDtypeStruct((nx * nc, nzh * nzl, 2 * cols), jnp.bfloat16),
            pltpu.VMEM(shape, jnp.bfloat16),
        ),
        in_specs=[SMEM] + [VMEM] * 6,
        out_specs=(VMEM, VMEM),
        name="project",
        compiler_params=params(12),
        cost_estimate=cost(4 * tokens * R * (D + cols), 10_000_000),
    )(place, mine, other, *near(xv, vv, xo, vo))


def summed_kernel(t, out, lines):
    total = jnp.sum(t[...].astype(jnp.float32), axis=0)
    nz, tiles, _ = out.shape
    for k in range(tiles):
        lines[pl.ds(k, nz, stride=tiles), :] = total[:, k * LANES : (k + 1) * LANES]
    out[...] = lines[...].reshape(out.shape).astype(jnp.bfloat16)


def summed(t):
    _, nz, width = t.shape
    tiles = width // LANES
    return pl.pallas_call(
        summed_kernel,
        out_shape=jax.ShapeDtypeStruct((nz, tiles, LANES), jnp.bfloat16),
        in_specs=[VMEM],
        out_specs=VMEM,
        scratch_shapes=[pltpu.VMEM((nz * tiles, LANES), jnp.float32)],
        name="summed",
        compiler_params=params(2),
        cost_estimate=cost(t.size, 600_000),
    )(t)


def gram_kernel(factors, grams):
    for f in range(2):
        factor = factors[f].reshape(D, R)
        gram = dot(factor, factor, TN)
        high = gram.astype(jnp.bfloat16)
        grams[f, 0] = high
        grams[f, 1] = (gram - high.astype(jnp.float32)).astype(jnp.bfloat16)


def gram_of(factors):
    shape = (2, 2, R, R)
    return pl.pallas_call(
        gram_kernel,
        out_shape=pltpu.VMEM(shape, jnp.bfloat16),
        in_specs=[VMEM],
        out_specs=VMEM,
        name="gram",
        compiler_params=params(8),
        cost_estimate=cost(4 * D * R * R, 3_000_000),
    )(*near(factors))


def moments_kernel(t, fv, sv, fo, so, out, nfv, nsv, nfo, nso):
    low = jnp.sum(t[...].astype(jnp.float32), axis=0)
    half = low.shape[0] // 2
    directions = []
    for part, first, second, next_first, next_second in (
        (low[:half], fv, sv, nfv, nsv),
        (low[half:], fo, so, nfo, nso),
    ):
        a = 0.9 * first[...] + 0.1 * part
        b = 0.95 * second[...] + 0.05 * part * part
        next_first[...] = a
        next_second[...] = b
        directions.append(a * lax.rsqrt(b))
    d = jnp.concatenate(directions, axis=0).astype(jnp.bfloat16)
    out[...] = jnp.broadcast_to(d[None], out.shape)


def moments(t, *state):
    shape = jax.ShapeDtypeStruct(state[0].shape, jnp.float32)
    return pl.pallas_call(
        moments_kernel,
        out_shape=(jax.ShapeDtypeStruct(t.shape, jnp.bfloat16), shape, shape, shape, shape),
        in_specs=[VMEM] * 5,
        out_specs=(VMEM,) * 5,
        name="moments",
        compiler_params=params(2),
        cost_estimate=cost(100_000, 150_000),
    )(t, *state)


def total_kernel(d, gram, out, whole, lines):
    tiles = d.shape[1]
    half = tiles // 2
    lines[...] = d[...].astype(jnp.float32).reshape(lines.shape)
    parts = [lines[pl.ds(k, R, stride=tiles), :].astype(jnp.bfloat16) for k in range(tiles)]
    rows = out.shape[1] // 2
    for f in range(2):
        part = jnp.concatenate(parts[f * half : (f + 1) * half], axis=1)
        whole[f] = part
        square = part.astype(jnp.float32) * (dot(gram[f, 0], part) + dot(gram[f, 1], part))
        out[:, f * rows : (f + 1) * rows] = jnp.full(
            (out.shape[0], rows, LANES), jnp.sum(square)
        )


def totals_of(count, d, gram):
    _, tiles, _ = d.shape
    cols = tiles // 2 * LANES
    return pl.pallas_call(
        total_kernel,
        out_shape=(
            jax.ShapeDtypeStruct((count, 8, LANES), jnp.float32),
            pltpu.VMEM((2, R, cols), jnp.bfloat16),
        ),
        in_specs=[VMEM, VMEM],
        out_specs=(VMEM, VMEM),
        scratch_shapes=[pltpu.VMEM((R * tiles, LANES), jnp.float32)],
        name="totals",
        compiler_params=params(6),
        cost_estimate=cost(8 * R * R * cols, 2_000_000),
    )(d, *near(gram))


def assemble_kernel(place, *refs):
    (*whole, _, out) = refs
    zl, x = place[1], place[3]
    nzh, nzl, nx = out.shape[:3]
    first = nzh // 2
    parts = [(k, s, part.at[s]) for k, part in enumerate(whole) for s in range(nzl)]
    for k, s, part in parts:
        px = lax.rem(x + nx - k, nx)
        at = lax.bitwise_xor(zl, s)
        for t in range(part.shape[1] - 1):
            lanes = slice(t * LANES, (t + 1) * LANES)
            out[first:, at, px, :, lanes] = part[: nzh - first, 1 + t]
            out[:first, at, px, :, lanes] = part[nzh - first :, 1 + t]


def assembled(place, parts, sizes, after):
    nzh, nzl, nx, _ = sizes
    tiles, rows = parts[0].shape[2:4]
    shape = (nzh, nzl, nx, rows, (tiles - 1) * LANES)
    return pl.pallas_call(
        assemble_kernel,
        out_shape=jax.ShapeDtypeStruct(shape, jnp.bfloat16),
        in_specs=[SMEM] + [VMEM] * len(parts) + [pl.BlockSpec(memory_space=pl.ANY)],
        out_specs=VMEM,
        name="assemble",
        compiler_params=params(8),
        cost_estimate=cost(1_000_000, 4_000_000),
    )(place, *near(*parts), after)


def final_kernel(place, totals, directions, factors, mine, other, ov, oo, *refs):
    copy_v, copy_o, sv, so, nv, no, out_v, out_o, own, sems = refs
    steps, nzl, nx, nc, rows, _ = factors.shape[1:]
    chunk = D // steps
    cols = directions.shape[2]
    sums = jnp.sum(totals[...], axis=0)
    scale = lax.rsqrt(sums / (D * WIDTH) + 1e-06)
    scales = scale[:1, :1], scale[4:5, :1]
    writes = []
    for k in range(2):
        part = pl.ds(k * steps // 2, steps // 2)
        lanes = pl.ds(k * D // 2, D // 2)
        writes += [
            pltpu.make_async_copy(out_v.at[part], copy_v.at[part], sems.at[2 * k]),
            pltpu.make_async_copy(out_o.at[:, lanes], copy_o.at[:, lanes], sems.at[2 * k + 1]),
        ]

    small = []
    for f, (w, targets) in enumerate(((ov, (sv, nv)), (oo, (so, no)))):
        mine_f = factors[f, place[4], place[1], place[3], place[2]]
        step = dot(mine_f, directions[f]) * scales[f]
        own[2 * f] = step
        own[2 * f + 1] = w[...] - 0.02 * step
        small += [
            pltpu.make_async_copy(own.at[2 * f + k], target, sems.at[4 + 2 * f + k])
            for k, target in enumerate(targets)
        ]
    for copy in small:
        copy.start()

    def copies(pair):
        for i in range(steps):
            for c in range(nc):
                factor = factors[0, i, :, :, c].reshape(chunk // nc, R)
                update = dot(factor, directions[0]) * (0.02 * scales[0])
                w = pair[c][i, :, :, :, :cols].reshape(chunk // nc, cols).astype(jnp.float32)
                out_v[i, :, :, c] = (w - update).astype(jnp.bfloat16).reshape(nzl, nx, rows, cols)
            if (i + 1) * 2 % steps == 0:
                writes[(i + 1) * 4 // steps - 2].start()
            update = dot(factors[1, i].reshape(chunk, R), directions[1]) * (0.02 * scales[1])
            w = jnp.stack([p[i, :, :, :, cols:] for p in pair], axis=2).reshape(chunk, cols)
            half = (w.astype(jnp.float32) - update).astype(jnp.bfloat16)
            out_o[:, i * chunk : (i + 1) * chunk] = half.T
            if (i + 1) * 2 % steps == 0:
                writes[(i + 1) * 4 // steps - 1].start()

    first = place[2] == 0

    @pl.when(first)
    def _():
        copies((mine, other))

    @pl.when(jnp.logical_not(first))
    def _():
        copies((other, mine))

    for copy in small + writes:
        copy.wait()


def final(place, totals, directions, factors, mine, other, ov, oo):
    cols = directions.shape[2]
    own = pltpu.HBM(ov.shape, jnp.float32)
    shape = (*factors.shape[1:-1], cols)
    copy_value, *rest = pl.pallas_call(
        final_kernel,
        out_shape=(
            pltpu.HBM(shape, jnp.bfloat16),
            pltpu.HBM((cols, D), jnp.bfloat16),
            own,
            own,
            own,
            own,
        ),
        in_specs=[SMEM] + [VMEM] * 7,
        out_specs=(HBM,) * 6,
        scratch_shapes=[
            pltpu.VMEM(shape, jnp.bfloat16),
            pltpu.VMEM((cols, D), jnp.bfloat16),
            pltpu.VMEM((4, *ov.shape), jnp.float32),
            pltpu.SemaphoreType.DMA((8,)),
        ],
        name="final",
        compiler_params=params(12),
        cost_estimate=cost(4 * D * cols * R, 10_000_000),
    )(place, totals, *near(directions, factors, mine, other), ov, oo)
    return copy_value.reshape(D, cols), *rest


def step(
    normed_input,
    value_cotangent,
    gated_output,
    layer_cotangent,
    factor_value,
    factor_output,
    weight_value,
    weight_output,
    first_value,
    second_value,
    first_output,
    second_output,
):
    nz, nx, nc = (lax.axis_size(a) for a in FS)
    nzh, nzl = nz // NZL, NZL
    sizes = nzh, nzl, nx, nc
    ny = lax.axis_size("tp")
    around = [turned(nz, nz // 2)]
    _, cols = weight_value.shape

    z = lax.axis_index("z")
    at = [lax.axis_index("tp"), z % nzl, lax.axis_index("c"), lax.axis_index("x"), z // nzl]
    place = jnp.stack(at).astype(jnp.int32)
    turned_weight = weight_output.T
    w, value_near, output_near = packed(
        nzh,
        place,
        factor_value,
        factor_output,
        weight_value,
        turned_weight,
        value_cotangent,
        gated_output,
    )
    w = exchange(w, "z", far_z(nz))
    f = to_all(w[:, 0], "z", near_z(nz))
    f = to_all(f, ("x", "tp"))
    other = moved(f, "c", 1)

    get = swapped(w, "z", 1)
    w = jnp.stack([w, get])
    get = swapped(w, "z", 2)
    w0 = jnp.concatenate([w, get])

    terms, factors = projected_terms(
        place, f, other, normed_input, value_near, layer_cotangent, output_near, sizes
    )
    t = exchange(terms, ("x", "c"))
    t = summed(t)
    t = exchange(t, "z", around)
    gram = gram_of(factors)

    w1 = moved(w0, "x", 1)
    w3 = moved(w0, "x", nx - 1)

    narrow = (cols // LANES, LANES)
    d, *state = moments(
        t,
        *(s.reshape(narrow) for s in (first_value, second_value, first_output, second_output)),
    )
    next_first_value, next_second_value, next_first_output, next_second_output = (
        s.reshape(1, cols) for s in state
    )
    d = exchange(d, "z", around)

    w2 = moved(w1, "x", 1)
    d = to_all(d, ("x", "c"))
    mine = assembled(place, (w0, w1, w2, w3), sizes, d)
    flip = moved(mine, "c", 1)

    totals, directions = totals_of(ny, d.reshape(R, *d.shape[2:]), gram)
    totals = exchange(totals, "tp")

    copy_value, copy_output, step_value, step_output, next_value, next_output = final(
        place,
        totals,
        directions,
        factors,
        mine,
        flip,
        weight_value,
        turned_weight,
    )
    return (
        step_value,
        step_output.T,
        next_value,
        next_output.T,
        next_first_value,
        next_second_value,
        next_first_output,
        next_second_output,
        copy_value,
        copy_output,
    )


def solution(mesh):
    torus = Mesh(mesh.devices.reshape(32, 4, 2, mesh.shape["tp"]), ("z", "x", "c", "tp"))
    placed = (
        P(FS, None),
        P(FS, "tp"),
        P(FS, "tp"),
        P(FS, None),
        P(FS, None),
        P(FS, None),
        P(FS, "tp"),
        P("tp", FS),
        P(FS, "tp"),
        P(FS, "tp"),
        P(FS, "tp"),
        P(FS, "tp"),
    )
    return jax.shard_map(
        step,
        mesh=torus,
        in_specs=placed,
        out_specs=(
            P(FS, "tp"),
            P("tp", FS),
            P(FS, "tp"),
            P("tp", FS),
            P(FS, "tp"),
            P(FS, "tp"),
            P(FS, "tp"),
            P(FS, "tp"),
            P(None, "tp"),
            P("tp", None),
        ),
        check_vma=False,
    )
```

```python
import jax
import jax.numpy as jnp
from jax import lax
from jax.experimental import pallas as pl
from jax.experimental.pallas import tpu as pltpu
from jax.sharding import Mesh
from jax.sharding import PartitionSpec as P

D = 2048
WIDTH = 2048
R = 256
FS = ("z", "x", "c")
NZL = 4
FIRST = 5
LANES = 128
TN = (((0,), (0,)), ((), ()))


VMEM = pl.BlockSpec(memory_space=pltpu.VMEM)
HBM = pl.BlockSpec(memory_space=pltpu.HBM)


def far(*arrays):
    return [pltpu.with_memory_space_constraint(a, pltpu.HBM) for a in arrays]


def near(*arrays):
    return [pltpu.with_memory_space_constraint(a, pltpu.VMEM) for a in arrays]


def params(mib):
    return pltpu.CompilerParams(vmem_limit_bytes=mib << 20)


def cost(flops, bytes_accessed):
    return pl.CostEstimate(flops=flops, bytes_accessed=bytes_accessed, transcendentals=0)


def dot(a, b, dims=(((1,), (0,)), ((), ()))):
    return lax.dot_general(a, b, dims, preferred_element_type=jnp.float32)


def turned(n, by):
    return [(i + by) % n for i in range(n)]


def near_z(nz):
    return [[i + k for k in (1, 0, 2, 3)] for i in range(0, nz, NZL)]


def far_z(nz):
    n = nz // NZL
    return [[i + NZL * k for k in turned(n, FIRST)] for i in range(NZL)]


def exchange(blocks, axes, groups=None):
    return lax.all_to_all(
        blocks, axes, split_axis=0, concat_axis=0, axis_index_groups=groups, tiled=True
    )


def to_all(block, axes, groups=None):
    count = len(groups[0]) if groups else lax.axis_size(axes)
    copies = jnp.broadcast_to(block[None], (count, *block.shape))
    return exchange(copies, axes, groups)


def moved(block, axis, by):
    n = lax.axis_size(axis)
    return lax.ppermute(block, axis, [(i, (i + by) % n) for i in range(n)])


def swapped(block, axis, bit):
    return lax.ppermute(block, axis, [(i, i ^ bit) for i in range(lax.axis_size(axis))])


def pack_kernel(fv, fo, wv, wo, out, fv_in, fo_in, wv_in, wo_in, sems):
    copies = [
        pltpu.make_async_copy(src, dst, sems.at[i])
        for i, (src, dst) in enumerate(((fv, fv_in), (fo, fo_in), (wv, wv_in), (wo, wo_in)))
    ]
    for copy in copies:
        copy.start()
    n = R // 8
    y = lax.axis_index("tp")
    j = lax.broadcasted_iota(jnp.int32, (R, R), 0)
    k = lax.broadcasted_iota(jnp.int32, (R, R), 1)
    turn = (j == (k % n + FIRST * NZL) % n * 8 + k // n).astype(jnp.bfloat16)
    for copy in copies:
        copy.wait()
    factor = jnp.where(y < 2, fv_in[...].astype(jnp.float32), fo_in[...].astype(jnp.float32))
    factor = dot(factor.astype(jnp.bfloat16), turn)
    tile = jnp.where(y % 2 == 0, factor[:, :LANES], factor[:, LANES:]).astype(jnp.bfloat16)
    tiles = [tile]
    for w in (wv_in, wo_in):
        half = w[...].astype(jnp.bfloat16)
        tiles += [half[:, t : t + LANES] for t in range(0, half.shape[1], LANES)]
    for t, tile in enumerate(tiles):
        out[:, t] = jnp.broadcast_to(tile[None], (out.shape[0], *tile.shape))


def packed(count, fv, fo, wv, wo):
    rows, cols = wv.shape
    tiles = 1 + 2 * cols // LANES
    return pl.pallas_call(
        pack_kernel,
        out_shape=jax.ShapeDtypeStruct((count, tiles, rows, LANES), jnp.bfloat16),
        in_specs=[HBM] * 4,
        out_specs=VMEM,
        scratch_shapes=[
            pltpu.VMEM(fv.shape, fv.dtype),
            pltpu.VMEM(fo.shape, fo.dtype),
            pltpu.VMEM(wv.shape, wv.dtype),
            pltpu.VMEM(wo.shape, wo.dtype),
            pltpu.SemaphoreType.DMA((4,)),
        ],
        name="packed",
        compiler_params=params(4),
        cost_estimate=cost(2 * 8 * R * R, 200_000),
    )(*far(fv, fo, wv, wo))


def project_kernel(mine, other, xv, vv, xo, vo, out, whole, late, sems):
    c = lax.axis_index("c")
    read = pltpu.make_async_copy(xo, late, sems.at[0])
    read.start()
    nzh, nzl, nx = whole.shape[1:4]
    first = FIRST
    half = R // LANES
    cols = vv.shape[1]
    for f in range(2):
        for src, at in ((mine, c), (other, 1 - c)):
            for x in range(nx):
                for h in range(half):
                    for k, zl in enumerate(near_z(nzl)[0]):
                        lanes = slice(h * LANES, (h + 1) * LANES)
                        block = src.at[x * 2 * half + f * half + h, k]
                        whole[f, first:, zl, x, at, :, lanes] = block[: nzh - first]
                        whole[f, :first, zl, x, at, :, lanes] = block[nzh - first :]
    for f, (x, v) in enumerate(((xv, vv), (late, vo))):
        if f == 1:
            read.wait()
        projected = dot(x[...], whole[f].reshape(D, R)).astype(jnp.bfloat16)
        term = dot(projected, v[...], TN).astype(jnp.bfloat16)
        out[:, :, f * cols : (f + 1) * cols] = term.reshape(out.shape[0], out.shape[1], cols)


def projected_terms(mine, other, xv, vv, xo, vo, sizes):
    nzh, nzl, nx, nc = sizes
    shape = (2, nzh, nzl, nx, nc, D // (nzh * nzl * nx * nc), R)
    cols = vv.shape[1]
    tokens = xv.shape[0]
    return pl.pallas_call(
        project_kernel,
        out_shape=(
            jax.ShapeDtypeStruct((nx * nc, nzh * nzl, 2 * cols), jnp.bfloat16),
            pltpu.VMEM(shape, jnp.bfloat16),
        ),
        in_specs=[VMEM] * 4 + [HBM, VMEM],
        out_specs=(VMEM, VMEM),
        scratch_shapes=[pltpu.VMEM(xo.shape, xo.dtype), pltpu.SemaphoreType.DMA((1,))],
        name="project",
        compiler_params=params(12),
        cost_estimate=cost(4 * tokens * R * (D + cols), 10_000_000),
    )(mine, other, *near(xv, vv), *far(xo), *near(vo))


def summed_kernel(t, out, lines):
    total = jnp.sum(t[...].astype(jnp.float32), axis=0)
    nz, tiles, _ = out.shape
    for k in range(tiles):
        lines[pl.ds(k, nz, stride=tiles), :] = total[:, k * LANES : (k + 1) * LANES]
    out[...] = lines[...].reshape(out.shape).astype(jnp.bfloat16)


def summed(t):
    _, nz, width = t.shape
    tiles = width // LANES
    return pl.pallas_call(
        summed_kernel,
        out_shape=jax.ShapeDtypeStruct((nz, tiles, LANES), jnp.bfloat16),
        in_specs=[VMEM],
        out_specs=VMEM,
        scratch_shapes=[pltpu.VMEM((nz * tiles, LANES), jnp.float32)],
        name="summed",
        compiler_params=params(2),
        cost_estimate=cost(t.size, 600_000),
    )(t)


def gram_kernel(factors, grams):
    for f in range(2):
        factor = factors[f].reshape(D, R)
        gram = dot(factor, factor, TN)
        high = gram.astype(jnp.bfloat16)
        grams[f, 0] = high
        grams[f, 1] = (gram - high.astype(jnp.float32)).astype(jnp.bfloat16)


def gram_of(factors):
    shape = (2, 2, R, R)
    return pl.pallas_call(
        gram_kernel,
        out_shape=pltpu.VMEM(shape, jnp.bfloat16),
        in_specs=[VMEM],
        out_specs=VMEM,
        name="gram",
        compiler_params=params(8),
        cost_estimate=cost(4 * D * R * R, 3_000_000),
    )(*near(factors))


def moments_kernel(t, fv, sv, fo, so, out, nfv, nsv, nfo, nso):
    low = jnp.sum(t[...].astype(jnp.float32), axis=0)
    half = low.shape[0] // 2
    directions = []
    for part, first, second, next_first, next_second in (
        (low[:half], fv, sv, nfv, nsv),
        (low[half:], fo, so, nfo, nso),
    ):
        a = 0.9 * first[...] + 0.1 * part
        b = 0.95 * second[...] + 0.05 * part * part
        next_first[...] = a
        next_second[...] = b
        directions.append(a * lax.rsqrt(b))
    d = jnp.concatenate(directions, axis=0).astype(jnp.bfloat16)
    out[...] = jnp.broadcast_to(d[None], out.shape)


def moments(t, *state):
    shape = jax.ShapeDtypeStruct(state[0].shape, jnp.float32)
    return pl.pallas_call(
        moments_kernel,
        out_shape=(jax.ShapeDtypeStruct(t.shape, jnp.bfloat16), shape, shape, shape, shape),
        in_specs=[VMEM] * 5,
        out_specs=(VMEM,) * 5,
        name="moments",
        compiler_params=params(2),
        cost_estimate=cost(100_000, 150_000),
    )(t, *state)


def total_kernel(d, gram, out, whole, lines):
    tiles = d.shape[1]
    half = tiles // 2
    lines[...] = d[...].astype(jnp.float32).reshape(lines.shape)
    parts = [lines[pl.ds(k, R, stride=tiles), :].astype(jnp.bfloat16) for k in range(tiles)]
    rows = out.shape[1] // 2
    for f in range(2):
        part = jnp.concatenate(parts[f * half : (f + 1) * half], axis=1)
        whole[f] = part
        square = part.astype(jnp.float32) * (dot(gram[f, 0], part) + dot(gram[f, 1], part))
        out[:, f * rows : (f + 1) * rows] = jnp.full(
            (out.shape[0], rows, LANES), jnp.sum(square)
        )


def totals_of(count, d, gram):
    _, tiles, _ = d.shape
    cols = tiles // 2 * LANES
    return pl.pallas_call(
        total_kernel,
        out_shape=(
            jax.ShapeDtypeStruct((count, 8, LANES), jnp.float32),
            pltpu.VMEM((2, R, cols), jnp.bfloat16),
        ),
        in_specs=[VMEM, VMEM],
        out_specs=(VMEM, VMEM),
        scratch_shapes=[pltpu.VMEM((R * tiles, LANES), jnp.float32)],
        name="totals",
        compiler_params=params(6),
        cost_estimate=cost(8 * R * R * cols, 2_000_000),
    )(d, *near(gram))


def assemble_kernel(*refs):
    (*whole, _, out) = refs
    zl, x = lax.axis_index("z") % NZL, lax.axis_index("x")
    nzh, nzl, nx = out.shape[:3]
    first = FIRST
    parts = [(k, s, part.at[s]) for k, part in enumerate(whole) for s in range(nzl)]
    for k, s, part in parts:
        px = lax.rem(x + nx - k, nx)
        at = lax.bitwise_xor(zl, s)
        for t in range(part.shape[1] - 1):
            lanes = slice(t * LANES, (t + 1) * LANES)
            out[first:, at, px, :, lanes] = part[: nzh - first, 1 + t]
            out[:first, at, px, :, lanes] = part[nzh - first :, 1 + t]


def assembled(parts, sizes, after):
    nzh, nzl, nx, _ = sizes
    tiles, rows = parts[0].shape[2:4]
    shape = (nzh, nzl, nx, rows, (tiles - 1) * LANES)
    return pl.pallas_call(
        assemble_kernel,
        out_shape=jax.ShapeDtypeStruct(shape, jnp.bfloat16),
        in_specs=[VMEM] * len(parts) + [pl.BlockSpec(memory_space=pl.ANY)],
        out_specs=VMEM,
        name="assemble",
        compiler_params=params(8),
        cost_estimate=cost(1_000_000, 4_000_000),
    )(*near(*parts), after)


def final_kernel(totals, directions, factors, mine, other, ov, oo, *refs):
    copy_v, copy_o, sv, so, nv, no, out_v, out_o, own, sems = refs
    steps, nzl, nx, nc, rows, _ = factors.shape[1:]
    chunk = D // steps
    cols = directions.shape[2]
    sums = jnp.sum(totals[...], axis=0)
    scale = lax.rsqrt(sums / (D * WIDTH) + 1e-06)
    scales = scale[:1, :1], scale[4:5, :1]
    writes = []
    for k in range(2):
        part = pl.ds(k * steps // 2, steps // 2)
        lanes = pl.ds(k * D // 2, D // 2)
        writes += [
            pltpu.make_async_copy(out_v.at[part], copy_v.at[part], sems.at[2 * k]),
            pltpu.make_async_copy(out_o.at[:, lanes], copy_o.at[:, lanes], sems.at[2 * k + 1]),
        ]

    z, x, c = (lax.axis_index(a) for a in FS)
    small = []
    for f, (w, targets) in enumerate(((ov, (sv, nv)), (oo, (so, no)))):
        factor = factors[f, z // NZL, z % NZL, x, c]
        step = dot(factor, directions[f]) * scales[f]
        own[2 * f] = step
        own[2 * f + 1] = w[...] - 0.02 * step
        small += [
            pltpu.make_async_copy(own.at[2 * f + k], target, sems.at[4 + 2 * f + k])
            for k, target in enumerate(targets)
        ]
    for copy in small:
        copy.start()

    def copies(pair):
        for i in range(steps):
            for k in range(nc):
                factor = factors[0, i, :, :, k].reshape(chunk // nc, R)
                update = dot(factor, directions[0]) * (0.02 * scales[0])
                w = pair[k][i, :, :, :, :cols].reshape(chunk // nc, cols).astype(jnp.float32)
                out_v[i, :, :, k] = (w - update).astype(jnp.bfloat16).reshape(nzl, nx, rows, cols)
            if (i + 1) * 2 % steps == 0:
                writes[(i + 1) * 4 // steps - 2].start()
            update = dot(factors[1, i].reshape(chunk, R), directions[1]) * (0.02 * scales[1])
            w = jnp.stack([p[i, :, :, :, cols:] for p in pair], axis=2).reshape(chunk, cols)
            half = (w.astype(jnp.float32) - update).astype(jnp.bfloat16)
            out_o[:, i * chunk : (i + 1) * chunk] = half.T
            if (i + 1) * 2 % steps == 0:
                writes[(i + 1) * 4 // steps - 1].start()

    first = c == 0

    @pl.when(first)
    def _():
        copies((mine, other))

    @pl.when(jnp.logical_not(first))
    def _():
        copies((other, mine))

    for copy in small + writes:
        copy.wait()


def final(totals, directions, factors, mine, other, ov, oo):
    cols = directions.shape[2]
    own = pltpu.HBM(ov.shape, jnp.float32)
    shape = (*factors.shape[1:-1], cols)
    copy_value, *rest = pl.pallas_call(
        final_kernel,
        out_shape=(
            pltpu.HBM(shape, jnp.bfloat16),
            pltpu.HBM((cols, D), jnp.bfloat16),
            own,
            own,
            own,
            own,
        ),
        in_specs=[VMEM] * 7,
        out_specs=(HBM,) * 6,
        scratch_shapes=[
            pltpu.VMEM(shape, jnp.bfloat16),
            pltpu.VMEM((cols, D), jnp.bfloat16),
            pltpu.VMEM((4, *ov.shape), jnp.float32),
            pltpu.SemaphoreType.DMA((8,)),
        ],
        name="final",
        compiler_params=params(12),
        cost_estimate=cost(4 * D * cols * R, 10_000_000),
    )(totals, *near(directions, factors, mine, other), ov, oo)
    return copy_value.reshape(D, cols), *rest


def step(
    normed_input,
    value_cotangent,
    gated_output,
    layer_cotangent,
    factor_value,
    factor_output,
    weight_value,
    weight_output,
    first_value,
    second_value,
    first_output,
    second_output,
):
    nz, nx, nc = (lax.axis_size(a) for a in FS)
    nzh, nzl = nz // NZL, NZL
    sizes = nzh, nzl, nx, nc
    ny = lax.axis_size("tp")
    around = [turned(nz, FIRST * NZL)]
    _, cols = weight_value.shape

    turned_weight = weight_output.T
    w = packed(nzh, factor_value, factor_output, weight_value, turned_weight)
    w = exchange(w, "z", far_z(nz))
    f = to_all(w[:, 0], "z", near_z(nz))
    f = to_all(f, ("x", "tp"))
    other = moved(f, "c", 1)

    get = swapped(w, "z", 1)
    w = jnp.stack([w, get])
    get = swapped(w, "z", 2)
    w0 = jnp.concatenate([w, get])

    terms, factors = projected_terms(
        f, other, normed_input, value_cotangent, layer_cotangent, gated_output, sizes
    )
    t = exchange(terms, ("x", "c"))
    t = summed(t)
    t = exchange(t, "z", around)
    gram = gram_of(factors)

    w1 = moved(w0, "x", 1)
    w3 = moved(w0, "x", nx - 1)

    narrow = (cols // LANES, LANES)
    d, *state = moments(
        t,
        *(s.reshape(narrow) for s in (first_value, second_value, first_output, second_output)),
    )
    next_first_value, next_second_value, next_first_output, next_second_output = (
        s.reshape(1, cols) for s in state
    )
    d = exchange(d, "z", around)

    w2 = moved(w1, "x", 1)
    d = to_all(d, ("x", "c"))
    mine = assembled((w0, w1, w2, w3), sizes, d)
    flip = moved(mine, "c", 1)

    totals, directions = totals_of(ny, d.reshape(R, *d.shape[2:]), gram)
    totals = exchange(totals, "tp")

    copy_value, copy_output, step_value, step_output, next_value, next_output = final(
        totals,
        directions,
        factors,
        mine,
        flip,
        weight_value,
        turned_weight,
    )
    return (
        step_value,
        step_output.T,
        next_value,
        next_output.T,
        next_first_value,
        next_second_value,
        next_first_output,
        next_second_output,
        copy_value,
        copy_output,
    )


def solution(mesh):
    torus = Mesh(mesh.devices.reshape(32, 4, 2, mesh.shape["tp"]), ("z", "x", "c", "tp"))
    placed = (
        P(FS, None),
        P(FS, "tp"),
        P(FS, "tp"),
        P(FS, None),
        P(FS, None),
        P(FS, None),
        P(FS, "tp"),
        P("tp", FS),
        P(FS, "tp"),
        P(FS, "tp"),
        P(FS, "tp"),
        P(FS, "tp"),
    )
    return jax.shard_map(
        step,
        mesh=torus,
        in_specs=placed,
        out_specs=(
            P(FS, "tp"),
            P("tp", FS),
            P(FS, "tp"),
            P("tp", FS),
            P(FS, "tp"),
            P(FS, "tp"),
            P(FS, "tp"),
            P(FS, "tp"),
            P(None, "tp"),
            P("tp", None),
        ),
        check_vma=False,
    )
```

```python
import jax
import jax.numpy as jnp
from jax import lax
from jax.experimental import pallas as pl
from jax.experimental.pallas import tpu as pltpu
from jax.sharding import Mesh
from jax.sharding import PartitionSpec as P

D = 2048
WIDTH = 2048
R = 256
FS = ("z", "x", "c")
PLANE = ("x", "c", "tp")
NZL = 4
FIRST = 5
LANES = 128
TN = (((0,), (0,)), ((), ()))


VMEM = pl.BlockSpec(memory_space=pltpu.VMEM)
HBM = pl.BlockSpec(memory_space=pltpu.HBM)


def far(*arrays):
    return [pltpu.with_memory_space_constraint(a, pltpu.HBM) for a in arrays]


def near(*arrays):
    return [pltpu.with_memory_space_constraint(a, pltpu.VMEM) for a in arrays]


def params(mib):
    return pltpu.CompilerParams(vmem_limit_bytes=mib << 20)


def cost(flops, bytes_accessed):
    return pl.CostEstimate(flops=flops, bytes_accessed=bytes_accessed, transcendentals=0)


def dot(a, b, dims=(((1,), (0,)), ((), ()))):
    return lax.dot_general(a, b, dims, preferred_element_type=jnp.float32)


def turned(n, by):
    return [(i + by) % n for i in range(n)]


def near_z(nz):
    return [[i + k for k in (1, 0, 2, 3)] for i in range(0, nz, NZL)]


def far_z(nz):
    n = nz // NZL
    return [[i + NZL * k for k in turned(n, FIRST)] for i in range(NZL)]


def plane_groups(nx, nc, ny):
    xs, ys = turned(nx, nx // 2), turned(ny, ny // 2)
    at = lambda x, c, y: (x * nc + c) * ny + y
    return (
        [[at(x, c, y) for x in xs for y in ys] for c in range(nc)],
        [[at(x, c, y) for x in xs for c in range(nc)] for y in range(ny)],
        [[at(x, c, y) for y in ys] for x in range(nx) for c in range(nc)],
    )


def exchange(blocks, axes, groups=None):
    return lax.all_to_all(
        blocks, axes, split_axis=0, concat_axis=0, axis_index_groups=groups, tiled=True
    )


def to_all(block, axes, groups=None):
    count = len(groups[0]) if groups else lax.axis_size(axes)
    copies = jnp.broadcast_to(block[None], (count, *block.shape))
    return exchange(copies, axes, groups)


def moved(block, axis, by):
    n = lax.axis_size(axis)
    return lax.ppermute(block, axis, [(i, (i + by) % n) for i in range(n)])


def swapped(block, axis, bit):
    return lax.ppermute(block, axis, [(i, i ^ bit) for i in range(lax.axis_size(axis))])


def pack_kernel(fv, fo, wv, wo, out, fv_in, fo_in, wv_in, wo_in, sems):
    copies = [
        pltpu.make_async_copy(src, dst, sems.at[i])
        for i, (src, dst) in enumerate(((fv, fv_in), (fo, fo_in), (wv, wv_in), (wo, wo_in)))
    ]
    for copy in copies:
        copy.start()
    n = R // 8
    y = lax.axis_index("tp")
    j = lax.broadcasted_iota(jnp.int32, (R, R), 0)
    k = lax.broadcasted_iota(jnp.int32, (R, R), 1)
    turn = (j == ((k % n + FIRST * NZL) % n * 8 + (k // n + 4) % 8)).astype(jnp.bfloat16)
    for copy in copies:
        copy.wait()
    factor = jnp.where(y < 2, fv_in[...].astype(jnp.float32), fo_in[...].astype(jnp.float32))
    factor = dot(factor.astype(jnp.bfloat16), turn)
    tile = jnp.where(y % 2 == 0, factor[:, :LANES], factor[:, LANES:]).astype(jnp.bfloat16)
    tiles = [tile]
    for w in (wv_in, wo_in):
        half = w[...].astype(jnp.bfloat16)
        tiles += [half[:, t : t + LANES] for t in range(0, half.shape[1], LANES)]
    for t, tile in enumerate(tiles):
        out[:, t] = jnp.broadcast_to(tile[None], (out.shape[0], *tile.shape))


def packed(count, fv, fo, wv, wo):
    rows, cols = wv.shape
    tiles = 1 + 2 * cols // LANES
    return pl.pallas_call(
        pack_kernel,
        out_shape=jax.ShapeDtypeStruct((count, tiles, rows, LANES), jnp.bfloat16),
        in_specs=[HBM] * 4,
        out_specs=VMEM,
        scratch_shapes=[
            pltpu.VMEM(fv.shape, fv.dtype),
            pltpu.VMEM(fo.shape, fo.dtype),
            pltpu.VMEM(wv.shape, wv.dtype),
            pltpu.VMEM(wo.shape, wo.dtype),
            pltpu.SemaphoreType.DMA((4,)),
        ],
        name="packed",
        compiler_params=params(4),
        cost_estimate=cost(2 * 8 * R * R, 200_000),
    )(*far(fv, fo, wv, wo))


def project_kernel(mine, other, xv, vv, xo, vo, out, whole, late, sems):
    c = lax.axis_index("c")
    read = pltpu.make_async_copy(xo, late, sems.at[0])
    read.start()
    nzh, nzl, nx = whole.shape[1:4]
    first = FIRST
    half = R // LANES
    cols = vv.shape[1]
    for f in range(2):
        for src, at in ((mine, c), (other, 1 - c)):
            for x in range(nx):
                for h in range(half):
                    for k, zl in enumerate(near_z(nzl)[0]):
                        lanes = slice(h * LANES, (h + 1) * LANES)
                        y = (f * half + h + half) % (2 * half)
                        block = src.at[(x + nx // 2) % nx * 2 * half + y, k]
                        whole[f, first:, zl, x, at, :, lanes] = block[: nzh - first]
                        whole[f, :first, zl, x, at, :, lanes] = block[nzh - first :]
    for f, (x, v) in enumerate(((xv, vv), (late, vo))):
        if f == 1:
            read.wait()
        projected = dot(x[...], whole[f].reshape(D, R)).astype(jnp.bfloat16)
        term = dot(projected, v[...], TN).astype(jnp.bfloat16)
        out[:, :, f * cols : (f + 1) * cols] = term.reshape(out.shape[0], out.shape[1], cols)


def projected_terms(mine, other, xv, vv, xo, vo, sizes):
    nzh, nzl, nx, nc = sizes
    shape = (2, nzh, nzl, nx, nc, D // (nzh * nzl * nx * nc), R)
    cols = vv.shape[1]
    tokens = xv.shape[0]
    return pl.pallas_call(
        project_kernel,
        out_shape=(
            jax.ShapeDtypeStruct((nx * nc, nzh * nzl, 2 * cols), jnp.bfloat16),
            pltpu.VMEM(shape, jnp.bfloat16),
        ),
        in_specs=[VMEM] * 4 + [HBM, VMEM],
        out_specs=(VMEM, VMEM),
        scratch_shapes=[pltpu.VMEM(xo.shape, xo.dtype), pltpu.SemaphoreType.DMA((1,))],
        name="project",
        compiler_params=params(12),
        cost_estimate=cost(4 * tokens * R * (D + cols), 10_000_000),
    )(mine, other, *near(xv, vv), *far(xo), *near(vo))


def summed_kernel(t, out, lines):
    total = jnp.sum(t[...].astype(jnp.float32), axis=0)
    nz, tiles, _ = out.shape
    for k in range(tiles):
        lines[pl.ds(k, nz, stride=tiles), :] = total[:, k * LANES : (k + 1) * LANES]
    out[...] = lines[...].reshape(out.shape).astype(jnp.bfloat16)


def summed(t):
    _, nz, width = t.shape
    tiles = width // LANES
    return pl.pallas_call(
        summed_kernel,
        out_shape=jax.ShapeDtypeStruct((nz, tiles, LANES), jnp.bfloat16),
        in_specs=[VMEM],
        out_specs=VMEM,
        scratch_shapes=[pltpu.VMEM((nz * tiles, LANES), jnp.float32)],
        name="summed",
        compiler_params=params(2),
        cost_estimate=cost(t.size, 600_000),
    )(t)


def gram_kernel(factors, grams):
    for f in range(2):
        factor = factors[f].reshape(D, R)
        gram = dot(factor, factor, TN)
        high = gram.astype(jnp.bfloat16)
        grams[f, 0] = high
        grams[f, 1] = (gram - high.astype(jnp.float32)).astype(jnp.bfloat16)


def gram_of(factors):
    shape = (2, 2, R, R)
    return pl.pallas_call(
        gram_kernel,
        out_shape=pltpu.VMEM(shape, jnp.bfloat16),
        in_specs=[VMEM],
        out_specs=VMEM,
        name="gram",
        compiler_params=params(8),
        cost_estimate=cost(4 * D * R * R, 3_000_000),
    )(*near(factors))


def moments_kernel(t, fv, sv, fo, so, out, nfv, nsv, nfo, nso):
    low = jnp.sum(t[...].astype(jnp.float32), axis=0)
    half = low.shape[0] // 2
    directions = []
    for part, first, second, next_first, next_second in (
        (low[:half], fv, sv, nfv, nsv),
        (low[half:], fo, so, nfo, nso),
    ):
        a = 0.9 * first[...] + 0.1 * part
        b = 0.95 * second[...] + 0.05 * part * part
        next_first[...] = a
        next_second[...] = b
        directions.append(a * lax.rsqrt(b))
    d = jnp.concatenate(directions, axis=0).astype(jnp.bfloat16)
    out[...] = jnp.broadcast_to(d[None], out.shape)


def moments(t, *state):
    shape = jax.ShapeDtypeStruct(state[0].shape, jnp.float32)
    return pl.pallas_call(
        moments_kernel,
        out_shape=(jax.ShapeDtypeStruct(t.shape, jnp.bfloat16), shape, shape, shape, shape),
        in_specs=[VMEM] * 5,
        out_specs=(VMEM,) * 5,
        name="moments",
        compiler_params=params(2),
        cost_estimate=cost(100_000, 150_000),
    )(t, *state)


def total_kernel(d, gram, out, whole, lines):
    tiles = d.shape[1]
    half = tiles // 2
    lines[...] = d[...].astype(jnp.float32).reshape(lines.shape)
    parts = [lines[pl.ds(k, R, stride=tiles), :].astype(jnp.bfloat16) for k in range(tiles)]
    rows = out.shape[1] // 2
    for f in range(2):
        part = jnp.concatenate(parts[f * half : (f + 1) * half], axis=1)
        whole[f] = part
        square = part.astype(jnp.float32) * (dot(gram[f, 0], part) + dot(gram[f, 1], part))
        out[:, f * rows : (f + 1) * rows] = jnp.full(
            (out.shape[0], rows, LANES), jnp.sum(square)
        )


def totals_of(count, d, gram):
    _, tiles, _ = d.shape
    cols = tiles // 2 * LANES
    return pl.pallas_call(
        total_kernel,
        out_shape=(
            jax.ShapeDtypeStruct((count, 8, LANES), jnp.float32),
            pltpu.VMEM((2, R, cols), jnp.bfloat16),
        ),
        in_specs=[VMEM, VMEM],
        out_specs=(VMEM, VMEM),
        scratch_shapes=[pltpu.VMEM((R * tiles, LANES), jnp.float32)],
        name="totals",
        compiler_params=params(6),
        cost_estimate=cost(8 * R * R * cols, 2_000_000),
    )(d, *near(gram))


def assemble_kernel(*refs):
    (*whole, _, out) = refs
    zl, x = lax.axis_index("z") % NZL, lax.axis_index("x")
    nzh, nzl, nx = out.shape[:3]
    first = FIRST
    parts = [(k, s, part.at[s]) for k, part in enumerate(whole) for s in range(nzl)]
    for k, s, part in parts:
        px = lax.rem(x + nx - k, nx)
        at = lax.bitwise_xor(zl, s)
        for t in range(part.shape[1] - 1):
            lanes = slice(t * LANES, (t + 1) * LANES)
            out[first:, at, px, :, lanes] = part[: nzh - first, 1 + t]
            out[:first, at, px, :, lanes] = part[nzh - first :, 1 + t]


def assembled(parts, sizes, after):
    nzh, nzl, nx, _ = sizes
    tiles, rows = parts[0].shape[2:4]
    shape = (nzh, nzl, nx, rows, (tiles - 1) * LANES)
    return pl.pallas_call(
        assemble_kernel,
        out_shape=jax.ShapeDtypeStruct(shape, jnp.bfloat16),
        in_specs=[VMEM] * len(parts) + [pl.BlockSpec(memory_space=pl.ANY)],
        out_specs=VMEM,
        name="assemble",
        compiler_params=params(8),
        cost_estimate=cost(1_000_000, 4_000_000),
    )(*near(*parts), after)


def final_kernel(totals, directions, factors, mine, other, ov, oo, *refs):
    copy_v, copy_o, sv, so, nv, no, out_v, out_o, own, sems = refs
    steps, nzl, nx, nc, rows, _ = factors.shape[1:]
    chunk = D // steps
    cols = directions.shape[2]
    sums = jnp.sum(totals[...], axis=0)
    scale = lax.rsqrt(sums / (D * WIDTH) + 1e-06)
    scales = scale[:1, :1], scale[4:5, :1]
    writes = []
    for k in range(2):
        part = pl.ds(k * steps // 2, steps // 2)
        lanes = pl.ds(k * D // 2, D // 2)
        writes += [
            pltpu.make_async_copy(out_v.at[part], copy_v.at[part], sems.at[2 * k]),
            pltpu.make_async_copy(out_o.at[:, lanes], copy_o.at[:, lanes], sems.at[2 * k + 1]),
        ]

    z, x, c = (lax.axis_index(a) for a in FS)
    small = []
    for f, (w, targets) in enumerate(((ov, (sv, nv)), (oo, (so, no)))):
        factor = factors[f, z // NZL, z % NZL, x, c]
        step = dot(factor, directions[f]) * scales[f]
        own[2 * f] = step
        own[2 * f + 1] = w[...] - 0.02 * step
        small += [
            pltpu.make_async_copy(own.at[2 * f + k], target, sems.at[4 + 2 * f + k])
            for k, target in enumerate(targets)
        ]
    for copy in small:
        copy.start()

    def copies(pair):
        for i in range(steps):
            for k in range(nc):
                factor = factors[0, i, :, :, k].reshape(chunk // nc, R)
                update = dot(factor, directions[0]) * (0.02 * scales[0])
                w = pair[k][i, :, :, :, :cols].reshape(chunk // nc, cols).astype(jnp.float32)
                out_v[i, :, :, k] = (w - update).astype(jnp.bfloat16).reshape(nzl, nx, rows, cols)
            if (i + 1) * 2 % steps == 0:
                writes[(i + 1) * 4 // steps - 2].start()
            update = dot(factors[1, i].reshape(chunk, R), directions[1]) * (0.02 * scales[1])
            w = jnp.stack([p[i, :, :, :, cols:] for p in pair], axis=2).reshape(chunk, cols)
            half = (w.astype(jnp.float32) - update).astype(jnp.bfloat16)
            out_o[:, i * chunk : (i + 1) * chunk] = half.T
            if (i + 1) * 2 % steps == 0:
                writes[(i + 1) * 4 // steps - 1].start()

    first = c == 0

    @pl.when(first)
    def _():
        copies((mine, other))

    @pl.when(jnp.logical_not(first))
    def _():
        copies((other, mine))

    for copy in small + writes:
        copy.wait()


def final(totals, directions, factors, mine, other, ov, oo):
    cols = directions.shape[2]
    own = pltpu.HBM(ov.shape, jnp.float32)
    shape = (*factors.shape[1:-1], cols)
    copy_value, *rest = pl.pallas_call(
        final_kernel,
        out_shape=(
            pltpu.HBM(shape, jnp.bfloat16),
            pltpu.HBM((cols, D), jnp.bfloat16),
            own,
            own,
            own,
            own,
        ),
        in_specs=[VMEM] * 7,
        out_specs=(HBM,) * 6,
        scratch_shapes=[
            pltpu.VMEM(shape, jnp.bfloat16),
            pltpu.VMEM((cols, D), jnp.bfloat16),
            pltpu.VMEM((4, *ov.shape), jnp.float32),
            pltpu.SemaphoreType.DMA((8,)),
        ],
        name="final",
        compiler_params=params(12),
        cost_estimate=cost(4 * D * cols * R, 10_000_000),
    )(totals, *near(directions, factors, mine, other), ov, oo)
    return copy_value.reshape(D, cols), *rest


def step(
    normed_input,
    value_cotangent,
    gated_output,
    layer_cotangent,
    factor_value,
    factor_output,
    weight_value,
    weight_output,
    first_value,
    second_value,
    first_output,
    second_output,
):
    nz, nx, nc = (lax.axis_size(a) for a in FS)
    nzh, nzl = nz // NZL, NZL
    sizes = nzh, nzl, nx, nc
    ny = lax.axis_size("tp")
    around = [turned(nz, FIRST * NZL)]
    over_xy, over_xc, over_y = plane_groups(nx, nc, ny)
    _, cols = weight_value.shape

    turned_weight = weight_output.T
    w = packed(nzh, factor_value, factor_output, weight_value, turned_weight)
    w = exchange(w, "z", far_z(nz))
    f = to_all(w[:, 0], "z", near_z(nz))
    f = to_all(f, PLANE, over_xy)
    other = moved(f, "c", 1)

    get = swapped(w, "z", 1)
    w = jnp.stack([w, get])
    get = swapped(w, "z", 2)
    w0 = jnp.concatenate([w, get])

    terms, factors = projected_terms(
        f, other, normed_input, value_cotangent, layer_cotangent, gated_output, sizes
    )
    t = exchange(terms, PLANE, over_xc)
    t = summed(t)
    t = exchange(t, "z", around)
    gram = gram_of(factors)

    w1 = moved(w0, "x", 1)
    w3 = moved(w0, "x", nx - 1)

    narrow = (cols // LANES, LANES)
    d, *state = moments(
        t,
        *(s.reshape(narrow) for s in (first_value, second_value, first_output, second_output)),
    )
    next_first_value, next_second_value, next_first_output, next_second_output = (
        s.reshape(1, cols) for s in state
    )
    d = exchange(d, "z", around)

    w2 = moved(w1, "x", 1)
    d = to_all(d, PLANE, over_xc)
    mine = assembled((w0, w1, w2, w3), sizes, d)
    flip = moved(mine, "c", 1)

    totals, directions = totals_of(ny, d.reshape(R, *d.shape[2:]), gram)
    totals = exchange(totals, PLANE, over_y)

    copy_value, copy_output, step_value, step_output, next_value, next_output = final(
        totals,
        directions,
        factors,
        mine,
        flip,
        weight_value,
        turned_weight,
    )
    return (
        step_value,
        step_output.T,
        next_value,
        next_output.T,
        next_first_value,
        next_second_value,
        next_first_output,
        next_second_output,
        copy_value,
        copy_output,
    )


def solution(mesh):
    torus = Mesh(mesh.devices.reshape(32, 4, 2, mesh.shape["tp"]), ("z", "x", "c", "tp"))
    placed = (
        P(FS, None),
        P(FS, "tp"),
        P(FS, "tp"),
        P(FS, None),
        P(FS, None),
        P(FS, None),
        P(FS, "tp"),
        P("tp", FS),
        P(FS, "tp"),
        P(FS, "tp"),
        P(FS, "tp"),
        P(FS, "tp"),
    )
    return jax.shard_map(
        step,
        mesh=torus,
        in_specs=placed,
        out_specs=(
            P(FS, "tp"),
            P("tp", FS),
            P(FS, "tp"),
            P("tp", FS),
            P(FS, "tp"),
            P(FS, "tp"),
            P(FS, "tp"),
            P(FS, "tp"),
            P(None, "tp"),
            P("tp", None),
        ),
        check_vma=False,
    )
```

```python
import jax
import jax.numpy as jnp
from jax import lax
from jax.experimental import pallas as pl
from jax.experimental.pallas import tpu as pltpu
from jax.sharding import Mesh
from jax.sharding import PartitionSpec as P

D = 2048
WIDTH = 2048
R = 256
FS = ("z", "x", "c")
PLANE = ("x", "c", "tp")
NZL = 4
FIRST = 5
LANES = 128
TN = (((0,), (0,)), ((), ()))


VMEM = pl.BlockSpec(memory_space=pltpu.VMEM)
HBM = pl.BlockSpec(memory_space=pltpu.HBM)


def far(*arrays):
    return [pltpu.with_memory_space_constraint(a, pltpu.HBM) for a in arrays]


def near(*arrays):
    return [pltpu.with_memory_space_constraint(a, pltpu.VMEM) for a in arrays]


def params(mib):
    return pltpu.CompilerParams(vmem_limit_bytes=mib << 20)


def cost(flops, bytes_accessed):
    return pl.CostEstimate(flops=flops, bytes_accessed=bytes_accessed, transcendentals=0)


def dot(a, b, dims=(((1,), (0,)), ((), ()))):
    return lax.dot_general(a, b, dims, preferred_element_type=jnp.float32)


def turned(n, by):
    return [(i + by) % n for i in range(n)]


def near_z(nz):
    return [[i + k for k in (1, 0, 2, 3)] for i in range(0, nz, NZL)]


def far_z(nz):
    n = nz // NZL
    return [[i + NZL * k for k in turned(n, FIRST)] for i in range(NZL)]


def plane_groups(nx, nc, ny):
    xs, ys = turned(nx, nx // 2), turned(ny, ny // 2)
    at = lambda x, c, y: (x * nc + c) * ny + y
    return (
        [[at(x, c, y) for x in xs for y in ys] for c in range(nc)],
        [[at(x, c, y) for x in xs for c in range(nc)] for y in range(ny)],
        [[at(x, c, y) for y in ys] for x in range(nx) for c in range(nc)],
    )


def column_of(k, nzh):
    slot = k // nzh % NZL
    near = jnp.where(slot < 2, 1 - slot, slot)
    z = (k % nzh + FIRST) % nzh * NZL + near
    return z * 8 + (k // (nzh * NZL) + 4) % 8


def exchange(blocks, axes, groups=None):
    return lax.all_to_all(
        blocks, axes, split_axis=0, concat_axis=0, axis_index_groups=groups, tiled=True
    )


def to_all(block, axes, groups=None):
    count = len(groups[0]) if groups else lax.axis_size(axes)
    copies = jnp.broadcast_to(block[None], (count, *block.shape))
    return exchange(copies, axes, groups)


def moved(block, axis, by):
    n = lax.axis_size(axis)
    return lax.ppermute(block, axis, [(i, (i + by) % n) for i in range(n)])


def swapped(block, axis, bit):
    return lax.ppermute(block, axis, [(i, i ^ bit) for i in range(lax.axis_size(axis))])


def pack_kernel(fv, fo, wv, wo, out, fv_in, fo_in, wv_in, wo_in, sems):
    copies = [
        pltpu.make_async_copy(src, dst, sems.at[i])
        for i, (src, dst) in enumerate(((fv, fv_in), (fo, fo_in), (wv, wv_in), (wo, wo_in)))
    ]
    for copy in copies:
        copy.start()
    n = R // 8
    y = lax.axis_index("tp")
    j = lax.broadcasted_iota(jnp.int32, (R, R), 0)
    k = lax.broadcasted_iota(jnp.int32, (R, R), 1)
    turn = (j == column_of(k, n // NZL)).astype(jnp.bfloat16)
    for copy in copies:
        copy.wait()
    factor = jnp.where(y < 2, fv_in[...].astype(jnp.float32), fo_in[...].astype(jnp.float32))
    factor = dot(factor.astype(jnp.bfloat16), turn)
    tile = jnp.where(y % 2 == 0, factor[:, :LANES], factor[:, LANES:]).astype(jnp.bfloat16)
    tiles = [tile]
    for w in (wv_in, wo_in):
        half = w[...].astype(jnp.bfloat16)
        tiles += [half[:, t : t + LANES] for t in range(0, half.shape[1], LANES)]
    for t, tile in enumerate(tiles):
        out[:, t] = jnp.broadcast_to(tile[None], (out.shape[0], *tile.shape))


def packed(count, fv, fo, wv, wo):
    rows, cols = wv.shape
    tiles = 1 + 2 * cols // LANES
    return pl.pallas_call(
        pack_kernel,
        out_shape=jax.ShapeDtypeStruct((count, tiles, rows, LANES), jnp.bfloat16),
        in_specs=[HBM] * 4,
        out_specs=VMEM,
        scratch_shapes=[
            pltpu.VMEM(fv.shape, fv.dtype),
            pltpu.VMEM(fo.shape, fo.dtype),
            pltpu.VMEM(wv.shape, wv.dtype),
            pltpu.VMEM(wo.shape, wo.dtype),
            pltpu.SemaphoreType.DMA((4,)),
        ],
        name="packed",
        compiler_params=params(4),
        cost_estimate=cost(2 * 8 * R * R, 200_000),
    )(*far(fv, fo, wv, wo))


def project_kernel(mine, other, xv, vv, xo, vo, out, whole, late, sems):
    c = lax.axis_index("c")
    read = pltpu.make_async_copy(xo, late, sems.at[0])
    read.start()
    nzh, nzl, nx = whole.shape[1:4]
    first = FIRST
    half = R // LANES
    cols = vv.shape[1]
    for f in range(2):
        for src, at in ((mine, c), (other, 1 - c)):
            for x in range(nx):
                for h in range(half):
                    for k, zl in enumerate(near_z(nzl)[0]):
                        lanes = slice(h * LANES, (h + 1) * LANES)
                        y = (f * half + h + half) % (2 * half)
                        block = src.at[(x + nx // 2) % nx * 2 * half + y, k]
                        whole[f, first:, zl, x, at, :, lanes] = block[: nzh - first]
                        whole[f, :first, zl, x, at, :, lanes] = block[nzh - first :]
    for f, (x, v) in enumerate(((xv, vv), (late, vo))):
        if f == 1:
            read.wait()
        projected = dot(x[...], whole[f].reshape(D, R)).astype(jnp.bfloat16)
        term = dot(projected, v[...], TN).astype(jnp.bfloat16)
        out[:, :, f * cols : (f + 1) * cols] = term.reshape(out.shape[0], out.shape[1], cols)


def projected_terms(mine, other, xv, vv, xo, vo, sizes):
    nzh, nzl, nx, nc = sizes
    shape = (2, nzh, nzl, nx, nc, D // (nzh * nzl * nx * nc), R)
    cols = vv.shape[1]
    tokens = xv.shape[0]
    return pl.pallas_call(
        project_kernel,
        out_shape=(
            jax.ShapeDtypeStruct((nx * nc, nzh * nzl, 2 * cols), jnp.bfloat16),
            pltpu.VMEM(shape, jnp.bfloat16),
        ),
        in_specs=[VMEM] * 4 + [HBM, VMEM],
        out_specs=(VMEM, VMEM),
        scratch_shapes=[pltpu.VMEM(xo.shape, xo.dtype), pltpu.SemaphoreType.DMA((1,))],
        name="project",
        compiler_params=params(12),
        cost_estimate=cost(4 * tokens * R * (D + cols), 10_000_000),
    )(mine, other, *near(xv, vv), *far(xo), *near(vo))


def summed_kernel(t, out):
    out[...] = jnp.sum(t[...].astype(jnp.float32), axis=0).reshape(out.shape)


def summed(t, nzh):
    _, nz, width = t.shape
    return pl.pallas_call(
        summed_kernel,
        out_shape=jax.ShapeDtypeStruct((nz // nzh, nzh, width), jnp.float32),
        in_specs=[VMEM],
        out_specs=VMEM,
        name="summed",
        compiler_params=params(2),
        cost_estimate=cost(t.size, 600_000),
    )(t)


def shared_kernel(t, fv, sv, fo, so, out):
    total = jnp.sum(t[...], axis=0)
    tiles = total.shape[1] // LANES
    first = 0.9 * jnp.concatenate([fv[...], fo[...]], axis=0)
    high = first.astype(jnp.bfloat16)
    low = (first - high.astype(jnp.float32)).astype(jnp.bfloat16)
    second = (0.95 * jnp.concatenate([sv[...], so[...]], axis=0)).astype(jnp.bfloat16)
    blocks = [total[:, k * LANES : (k + 1) * LANES].astype(jnp.bfloat16) for k in range(tiles)]
    for k, block in enumerate([*blocks, high, low, second]):
        out[:, k] = jnp.broadcast_to(block[None], (out.shape[0], *block.shape))


def shared(t, *state):
    _, nzh, width = t.shape
    shape = (nzh, width // LANES + 3, nzh, LANES)
    return pl.pallas_call(
        shared_kernel,
        out_shape=jax.ShapeDtypeStruct(shape, jnp.bfloat16),
        in_specs=[VMEM] * 5,
        out_specs=VMEM,
        name="shared",
        compiler_params=params(2),
        cost_estimate=cost(t.size, 400_000),
    )(t, *state)


def gram_kernel(factors, grams):
    for f in range(2):
        factor = factors[f].reshape(D, R)
        gram = dot(factor, factor, TN)
        high = gram.astype(jnp.bfloat16)
        grams[f, 0] = high
        grams[f, 1] = (gram - high.astype(jnp.float32)).astype(jnp.bfloat16)


def gram_of(factors):
    shape = (2, 2, R, R)
    return pl.pallas_call(
        gram_kernel,
        out_shape=pltpu.VMEM(shape, jnp.bfloat16),
        in_specs=[VMEM],
        out_specs=VMEM,
        name="gram",
        compiler_params=params(8),
        cost_estimate=cost(4 * D * R * R, 3_000_000),
    )(*near(factors))


def moments_kernel(t, fv, sv, fo, so, out, nfv, nsv, nfo, nso, lines):
    nzh = t.shape[0]
    tiles = t.shape[1] - 3
    states = []
    for k in range(3):
        lines[k] = t[:, tiles + k].astype(jnp.float32).reshape(nzh * tiles, LANES)
        states.append([lines[k, pl.ds(s, nzh, stride=tiles), :] for s in range(tiles)])
    mine = lax.rem(lax.axis_index("z") // NZL + nzh - FIRST, nzh)
    here = lax.broadcasted_iota(jnp.int32, (nzh, LANES), 0) == mine
    half = tiles // 2
    for k in range(tiles):
        low = jnp.sum(t[:, k].astype(jnp.float32), axis=0)
        first = states[0][k] + states[1][k] + 0.1 * low
        second = states[2][k] + 0.05 * low * low
        d = (first * lax.rsqrt(second)).astype(jnp.bfloat16)
        out[:, k] = jnp.broadcast_to(d[None], (out.shape[0], *d.shape))
        own = jnp.sum(jnp.where(here, low, 0.0), axis=0, keepdims=True)
        at = slice(k % half, k % half + 1)
        f, s, nf, ns = (fv, sv, nfv, nsv) if k < half else (fo, so, nfo, nso)
        nf[at] = 0.9 * f[at] + 0.1 * own
        ns[at] = 0.95 * s[at] + 0.05 * own * own


def moments(t, *state):
    nzh, tiles = t.shape[0], t.shape[1] - 3
    shape = jax.ShapeDtypeStruct(state[0].shape, jnp.float32)
    return pl.pallas_call(
        moments_kernel,
        out_shape=(
            jax.ShapeDtypeStruct((NZL, tiles, nzh, LANES), jnp.bfloat16),
            shape,
            shape,
            shape,
            shape,
        ),
        in_specs=[VMEM] * 5,
        out_specs=(VMEM,) * 5,
        scratch_shapes=[pltpu.VMEM((3, nzh * tiles, LANES), jnp.float32)],
        name="moments",
        compiler_params=params(2),
        cost_estimate=cost(300_000, 400_000),
    )(t, *state)


def total_kernel(d, gram, out, whole):
    tiles = d.shape[1]
    half = tiles // 2
    rows = out.shape[1] // 2
    for f in range(2):
        part = jnp.concatenate(
            [d[:, k].reshape(R, LANES) for k in range(f * half, (f + 1) * half)], axis=1
        )
        whole[f] = part
        square = part.astype(jnp.float32) * (dot(gram[f, 0], part) + dot(gram[f, 1], part))
        out[:, f * rows : (f + 1) * rows] = jnp.full(
            (out.shape[0], rows, LANES), jnp.sum(square)
        )


def totals_of(count, d, gram):
    tiles = d.shape[1]
    cols = tiles // 2 * LANES
    return pl.pallas_call(
        total_kernel,
        out_shape=(
            jax.ShapeDtypeStruct((count, 8, LANES), jnp.float32),
            pltpu.VMEM((2, R, cols), jnp.bfloat16),
        ),
        in_specs=[VMEM, VMEM],
        out_specs=(VMEM, VMEM),
        name="totals",
        compiler_params=params(6),
        cost_estimate=cost(8 * R * R * cols, 2_000_000),
    )(d, *near(gram))


def assemble_kernel(*refs):
    (*whole, _, out) = refs
    zl, x = lax.axis_index("z") % NZL, lax.axis_index("x")
    nzh, nzl, nx = out.shape[:3]
    first = FIRST
    parts = [(k, s, part.at[s]) for k, part in enumerate(whole) for s in range(nzl)]
    for k, s, part in parts:
        px = lax.rem(x + nx - k, nx)
        at = lax.bitwise_xor(zl, s)
        for t in range(part.shape[1]):
            lanes = slice(t * LANES, (t + 1) * LANES)
            out[first:, at, px, :, lanes] = part[: nzh - first, t]
            out[:first, at, px, :, lanes] = part[nzh - first :, t]


def assembled(parts, sizes, after):
    nzh, nzl, nx, _ = sizes
    tiles, rows = parts[0].shape[2:4]
    shape = (nzh, nzl, nx, rows, tiles * LANES)
    return pl.pallas_call(
        assemble_kernel,
        out_shape=jax.ShapeDtypeStruct(shape, jnp.bfloat16),
        in_specs=[VMEM] * len(parts) + [pl.BlockSpec(memory_space=pl.ANY)],
        out_specs=VMEM,
        name="assemble",
        compiler_params=params(8),
        cost_estimate=cost(1_000_000, 4_000_000),
    )(*near(*parts), after)


def final_kernel(totals, directions, factors, mine, other, ov, oo, *refs):
    copy_v, copy_o, sv, so, nv, no, out_v, out_o, own, sems = refs
    steps, nzl, nx, nc, rows, _ = factors.shape[1:]
    chunk = D // steps
    cols = directions.shape[2]
    sums = jnp.sum(totals[...], axis=0)
    scale = lax.rsqrt(sums / (D * WIDTH) + 1e-06)
    scales = scale[:1, :1], scale[4:5, :1]
    writes = []
    for k in range(2):
        part = pl.ds(k * steps // 2, steps // 2)
        lanes = pl.ds(k * D // 2, D // 2)
        writes += [
            pltpu.make_async_copy(out_v.at[part], copy_v.at[part], sems.at[2 * k]),
            pltpu.make_async_copy(out_o.at[:, lanes], copy_o.at[:, lanes], sems.at[2 * k + 1]),
        ]

    z, x, c = (lax.axis_index(a) for a in FS)
    small = []
    for f, (w, targets) in enumerate(((ov, (sv, nv)), (oo, (so, no)))):
        factor = factors[f, z // NZL, z % NZL, x, c]
        step = dot(factor, directions[f]) * scales[f]
        own[2 * f] = step
        own[2 * f + 1] = w[...] - 0.02 * step
        small += [
            pltpu.make_async_copy(own.at[2 * f + k], target, sems.at[4 + 2 * f + k])
            for k, target in enumerate(targets)
        ]
    for copy in small:
        copy.start()

    def copies(pair):
        for i in range(steps):
            for k in range(nc):
                factor = factors[0, i, :, :, k].reshape(chunk // nc, R)
                update = dot(factor, directions[0]) * (0.02 * scales[0])
                w = pair[k][i, :, :, :, :cols].reshape(chunk // nc, cols).astype(jnp.float32)
                out_v[i, :, :, k] = (w - update).astype(jnp.bfloat16).reshape(nzl, nx, rows, cols)
            if (i + 1) * 2 % steps == 0:
                writes[(i + 1) * 4 // steps - 2].start()
            update = dot(factors[1, i].reshape(chunk, R), directions[1]) * (0.02 * scales[1])
            w = jnp.stack([p[i, :, :, :, cols:] for p in pair], axis=2).reshape(chunk, cols)
            half = (w.astype(jnp.float32) - update).astype(jnp.bfloat16)
            out_o[:, i * chunk : (i + 1) * chunk] = half.T
            if (i + 1) * 2 % steps == 0:
                writes[(i + 1) * 4 // steps - 1].start()

    first = c == 0

    @pl.when(first)
    def _():
        copies((mine, other))

    @pl.when(jnp.logical_not(first))
    def _():
        copies((other, mine))

    for copy in small + writes:
        copy.wait()


def final(totals, directions, factors, mine, other, ov, oo):
    cols = directions.shape[2]
    own = pltpu.HBM(ov.shape, jnp.float32)
    shape = (*factors.shape[1:-1], cols)
    copy_value, *rest = pl.pallas_call(
        final_kernel,
        out_shape=(
            pltpu.HBM(shape, jnp.bfloat16),
            pltpu.HBM((cols, D), jnp.bfloat16),
            own,
            own,
            own,
            own,
        ),
        in_specs=[VMEM] * 7,
        out_specs=(HBM,) * 6,
        scratch_shapes=[
            pltpu.VMEM(shape, jnp.bfloat16),
            pltpu.VMEM((cols, D), jnp.bfloat16),
            pltpu.VMEM((4, *ov.shape), jnp.float32),
            pltpu.SemaphoreType.DMA((8,)),
        ],
        name="final",
        compiler_params=params(12),
        cost_estimate=cost(4 * D * cols * R, 10_000_000),
    )(totals, *near(directions, factors, mine, other), ov, oo)
    return copy_value.reshape(D, cols), *rest


def step(
    normed_input,
    value_cotangent,
    gated_output,
    layer_cotangent,
    factor_value,
    factor_output,
    weight_value,
    weight_output,
    first_value,
    second_value,
    first_output,
    second_output,
):
    nz, nx, nc = (lax.axis_size(a) for a in FS)
    nzh, nzl = nz // NZL, NZL
    sizes = nzh, nzl, nx, nc
    ny = lax.axis_size("tp")
    over_xy, over_xc, over_y = plane_groups(nx, nc, ny)
    _, cols = weight_value.shape

    turned_weight = weight_output.T
    w = packed(nzh, factor_value, factor_output, weight_value, turned_weight)
    w = exchange(w, "z", far_z(nz))
    f = to_all(w[:, 0], "z", near_z(nz))
    f = to_all(f, PLANE, over_xy)
    other = moved(f, "c", 1)

    get = swapped(w, "z", 1)
    w = jnp.stack([w, get])
    get = swapped(w, "z", 2)
    w0 = jnp.concatenate([w[:, :, 1:], get[:, :, 1:]])

    terms, factors = projected_terms(
        f, other, normed_input, value_cotangent, layer_cotangent, gated_output, sizes
    )
    t = exchange(terms, PLANE, over_xc)
    t = summed(t, nzh)
    w1 = moved(w0, "x", 1)
    w3 = moved(w0, "x", nx - 1)
    t = exchange(t, "z", near_z(nz))

    narrow = (cols // LANES, LANES)
    state = [s.reshape(narrow) for s in (first_value, second_value, first_output, second_output)]
    t = shared(t, *state)
    t = exchange(t, "z", far_z(nz))
    w2 = moved(w1, "x", 1)
    gram = gram_of(factors)
    d, *state = moments(t, *state)
    next_first_value, next_second_value, next_first_output, next_second_output = (
        s.reshape(1, cols) for s in state
    )
    d = exchange(d, "z", near_z(nz))
    d = to_all(d, PLANE, over_xc)
    mine = assembled((w0, w1, w2, w3), sizes, d)
    flip = moved(mine, "c", 1)

    totals, directions = totals_of(ny, d.reshape(-1, *d.shape[2:]), gram)
    totals = exchange(totals, PLANE, over_y)

    copy_value, copy_output, step_value, step_output, next_value, next_output = final(
        totals,
        directions,
        factors,
        mine,
        flip,
        weight_value,
        turned_weight,
    )
    return (
        step_value,
        step_output.T,
        next_value,
        next_output.T,
        next_first_value,
        next_second_value,
        next_first_output,
        next_second_output,
        copy_value,
        copy_output,
    )


def solution(mesh):
    torus = Mesh(mesh.devices.reshape(32, 4, 2, mesh.shape["tp"]), ("z", "x", "c", "tp"))
    placed = (
        P(FS, None),
        P(FS, "tp"),
        P(FS, "tp"),
        P(FS, None),
        P(FS, None),
        P(FS, None),
        P(FS, "tp"),
        P("tp", FS),
        P(FS, "tp"),
        P(FS, "tp"),
        P(FS, "tp"),
        P(FS, "tp"),
    )
    return jax.shard_map(
        step,
        mesh=torus,
        in_specs=placed,
        out_specs=(
            P(FS, "tp"),
            P("tp", FS),
            P(FS, "tp"),
            P("tp", FS),
            P(FS, "tp"),
            P(FS, "tp"),
            P(FS, "tp"),
            P(FS, "tp"),
            P(None, "tp"),
            P("tp", None),
        ),
        check_vma=False,
    )
```

```python
import jax
import jax.numpy as jnp
from jax import lax
from jax.experimental import pallas as pl
from jax.experimental.pallas import tpu as pltpu
from jax.sharding import Mesh
from jax.sharding import PartitionSpec as P

D = 2048
WIDTH = 2048
R = 256
FS = ("z", "x", "c")
PLANE = ("x", "c", "tp")
ALL = ("z", *PLANE)
NZL = 4
FIRST = 5
LANES = 128
TN = (((0,), (0,)), ((), ()))


VMEM = pl.BlockSpec(memory_space=pltpu.VMEM)
HBM = pl.BlockSpec(memory_space=pltpu.HBM)


def far(*arrays):
    return [pltpu.with_memory_space_constraint(a, pltpu.HBM) for a in arrays]


def near(*arrays):
    return [pltpu.with_memory_space_constraint(a, pltpu.VMEM) for a in arrays]


def params(mib):
    return pltpu.CompilerParams(vmem_limit_bytes=mib << 20)


def cost(flops, bytes_accessed):
    return pl.CostEstimate(flops=flops, bytes_accessed=bytes_accessed, transcendentals=0)


def dot(a, b, dims=(((1,), (0,)), ((), ()))):
    return lax.dot_general(a, b, dims, preferred_element_type=jnp.float32)


def turned(n, by):
    return [(i + by) % n for i in range(n)]


def near_z(nz):
    return [[i + k for k in (1, 0, 2, 3)] for i in range(0, nz, NZL)]


def far_z(nz):
    n = nz // NZL
    return [[i + NZL * k for k in turned(n, FIRST)] for i in range(NZL)]


def plane_groups(nx, nc, ny):
    xs, ys = turned(nx, nx // 2), turned(ny, ny // 2)
    at = lambda x, c, y: (x * nc + c) * ny + y
    return (
        [[at(x, c, y) for x in xs for y in ys] for c in range(nc)],
        [[at(x, c, y) for c in range(nc) for x in xs] for y in range(ny)],
        [[at(x, c, y) for y in ys] for x in range(nx) for c in range(nc)],
    )


def block_groups(nz, nx, nc, ny):
    return [
        [((z * nx + x) * nc + c) * ny + y for x in turned(nx, nx // 2) for z in near]
        for near in near_z(nz)
        for c in range(nc)
        for y in range(ny)
    ]


def column_of(k, nzh):
    slot = k // nzh % NZL
    near = jnp.where(slot < 2, 1 - slot, slot)
    z = (k % nzh + FIRST) % nzh * NZL + near
    place = k // (nzh * NZL)
    return z * 8 + (place + 2) % 4 * 2 + place // 4


def exchange(blocks, axes, groups=None):
    return lax.all_to_all(
        blocks, axes, split_axis=0, concat_axis=0, axis_index_groups=groups, tiled=True
    )


def to_all(block, axes, groups=None):
    count = len(groups[0]) if groups else lax.axis_size(axes)
    copies = jnp.broadcast_to(block[None], (count, *block.shape))
    return exchange(copies, axes, groups)


def moved(block, axis, by):
    n = lax.axis_size(axis)
    return lax.ppermute(block, axis, [(i, (i + by) % n) for i in range(n)])


def swapped(block, axis, bit):
    return lax.ppermute(block, axis, [(i, i ^ bit) for i in range(lax.axis_size(axis))])


def pack_kernel(fv, fo, wv, wo, out, fv_in, fo_in, wv_in, wo_in, sems):
    copies = [
        pltpu.make_async_copy(src, dst, sems.at[i])
        for i, (src, dst) in enumerate(((fv, fv_in), (fo, fo_in), (wv, wv_in), (wo, wo_in)))
    ]
    for copy in copies:
        copy.start()
    n = R // 8
    y = lax.axis_index("tp")
    j = lax.broadcasted_iota(jnp.int32, (R, R), 0)
    k = lax.broadcasted_iota(jnp.int32, (R, R), 1)
    turn = (j == column_of(k, n // NZL)).astype(jnp.bfloat16)
    for copy in copies:
        copy.wait()
    factor = jnp.where(y < 2, fv_in[...].astype(jnp.float32), fo_in[...].astype(jnp.float32))
    factor = dot(factor.astype(jnp.bfloat16), turn)
    tile = jnp.where(y % 2 == 0, factor[:, :LANES], factor[:, LANES:]).astype(jnp.bfloat16)
    tiles = [tile]
    for w in (wv_in, wo_in):
        half = w[...].astype(jnp.bfloat16)
        tiles += [half[:, t : t + LANES] for t in range(0, half.shape[1], LANES)]
    for t, tile in enumerate(tiles):
        out[:, t] = jnp.broadcast_to(tile[None], (out.shape[0], *tile.shape))


def packed(count, fv, fo, wv, wo):
    rows, cols = wv.shape
    tiles = 1 + 2 * cols // LANES
    return pl.pallas_call(
        pack_kernel,
        out_shape=jax.ShapeDtypeStruct((count, tiles, rows, LANES), jnp.bfloat16),
        in_specs=[HBM] * 4,
        out_specs=VMEM,
        scratch_shapes=[
            pltpu.VMEM(fv.shape, fv.dtype),
            pltpu.VMEM(fo.shape, fo.dtype),
            pltpu.VMEM(wv.shape, wv.dtype),
            pltpu.VMEM(wo.shape, wo.dtype),
            pltpu.SemaphoreType.DMA((4,)),
        ],
        name="packed",
        compiler_params=params(4),
        cost_estimate=cost(2 * 8 * R * R, 200_000),
    )(*far(fv, fo, wv, wo))


def project_kernel(mine, other, xv, vv, xo, vo, out, whole, late, sems):
    c = lax.axis_index("c")
    read = pltpu.make_async_copy(xo, late, sems.at[0])
    read.start()
    nzh, nzl, nx = whole.shape[1:4]
    first = FIRST
    half = R // LANES
    cols = vv.shape[1]
    for f in range(2):
        for src, at in ((mine, c), (other, 1 - c)):
            for x in range(nx):
                for h in range(half):
                    for k, zl in enumerate(near_z(nzl)[0]):
                        lanes = slice(h * LANES, (h + 1) * LANES)
                        y = (f * half + h + half) % (2 * half)
                        block = src.at[(x + nx // 2) % nx * 2 * half + y, k]
                        whole[f, first:, zl, x, at, :, lanes] = block[: nzh - first]
                        whole[f, :first, zl, x, at, :, lanes] = block[nzh - first :]
    for f, (x, v) in enumerate(((xv, vv), (late, vo))):
        if f == 1:
            read.wait()
        projected = dot(x[...], whole[f].reshape(D, R)).astype(jnp.bfloat16)
        term = dot(projected, v[...], TN).astype(jnp.bfloat16)
        out[:, :, f * cols : (f + 1) * cols] = term.reshape(out.shape[0], out.shape[1], cols)


def projected_terms(mine, other, xv, vv, xo, vo, sizes):
    nzh, nzl, nx, nc = sizes
    shape = (2, nzh, nzl, nx, nc, D // (nzh * nzl * nx * nc), R)
    cols = vv.shape[1]
    tokens = xv.shape[0]
    return pl.pallas_call(
        project_kernel,
        out_shape=(
            jax.ShapeDtypeStruct((nx * nc, nzh * nzl, 2 * cols), jnp.bfloat16),
            pltpu.VMEM(shape, jnp.bfloat16),
        ),
        in_specs=[VMEM] * 4 + [HBM, VMEM],
        out_specs=(VMEM, VMEM),
        scratch_shapes=[pltpu.VMEM(xo.shape, xo.dtype), pltpu.SemaphoreType.DMA((1,))],
        name="project",
        compiler_params=params(12),
        cost_estimate=cost(4 * tokens * R * (D + cols), 10_000_000),
    )(mine, other, *near(xv, vv), *far(xo), *near(vo))


def summed_kernel(t, out):
    out[...] = jnp.sum(t[...].astype(jnp.float32), axis=0).reshape(out.shape)


def summed(t, nzh):
    _, nz, width = t.shape
    return pl.pallas_call(
        summed_kernel,
        out_shape=jax.ShapeDtypeStruct((nz // nzh, nzh, width), jnp.float32),
        in_specs=[VMEM],
        out_specs=VMEM,
        name="summed",
        compiler_params=params(2),
        cost_estimate=cost(t.size, 600_000),
    )(t)


def shared_kernel(t, fv, sv, fo, so, out):
    total = jnp.sum(t[...], axis=0)
    tiles = total.shape[1] // LANES
    first = 0.9 * jnp.concatenate([fv[...], fo[...]], axis=0)
    high = first.astype(jnp.bfloat16)
    low = (first - high.astype(jnp.float32)).astype(jnp.bfloat16)
    second = (0.95 * jnp.concatenate([sv[...], so[...]], axis=0)).astype(jnp.bfloat16)
    blocks = [total[:, k * LANES : (k + 1) * LANES].astype(jnp.bfloat16) for k in range(tiles)]
    for k, block in enumerate([*blocks, high, low, second]):
        out[:, k] = jnp.broadcast_to(block[None], (out.shape[0], *block.shape))


def shared(t, *state):
    _, nzh, width = t.shape
    shape = (nzh, width // LANES + 3, nzh, LANES)
    return pl.pallas_call(
        shared_kernel,
        out_shape=jax.ShapeDtypeStruct(shape, jnp.bfloat16),
        in_specs=[VMEM] * 5,
        out_specs=VMEM,
        name="shared",
        compiler_params=params(2),
        cost_estimate=cost(t.size, 400_000),
    )(t, *state)


def gram_kernel(factors, grams):
    for f in range(2):
        factor = factors[f].reshape(D, R)
        gram = dot(factor, factor, TN)
        high = gram.astype(jnp.bfloat16)
        grams[f, 0] = high
        grams[f, 1] = (gram - high.astype(jnp.float32)).astype(jnp.bfloat16)


def gram_of(factors):
    shape = (2, 2, R, R)
    return pl.pallas_call(
        gram_kernel,
        out_shape=pltpu.VMEM(shape, jnp.bfloat16),
        in_specs=[VMEM],
        out_specs=VMEM,
        name="gram",
        compiler_params=params(8),
        cost_estimate=cost(4 * D * R * R, 3_000_000),
    )(*near(factors))


def moments_kernel(t, fv, sv, fo, so, out, nfv, nsv, nfo, nso, lines):
    nzh = t.shape[0]
    tiles = t.shape[1] - 3
    states = []
    for k in range(3):
        lines[k] = t[:, tiles + k].astype(jnp.float32).reshape(nzh * tiles, LANES)
        states.append([lines[k, pl.ds(s, nzh, stride=tiles), :] for s in range(tiles)])
    mine = lax.rem(lax.axis_index("z") // NZL + nzh - FIRST, nzh)
    here = lax.broadcasted_iota(jnp.int32, (nzh, LANES), 0) == mine
    half = tiles // 2
    for k in range(tiles):
        low = jnp.sum(t[:, k].astype(jnp.float32), axis=0)
        first = states[0][k] + states[1][k] + 0.1 * low
        second = states[2][k] + 0.05 * low * low
        d = (first * lax.rsqrt(second)).astype(jnp.bfloat16)
        out[:, k] = jnp.broadcast_to(d[None], (out.shape[0], *d.shape))
        own = jnp.sum(jnp.where(here, low, 0.0), axis=0, keepdims=True)
        at = slice(k % half, k % half + 1)
        f, s, nf, ns = (fv, sv, nfv, nsv) if k < half else (fo, so, nfo, nso)
        nf[at] = 0.9 * f[at] + 0.1 * own
        ns[at] = 0.95 * s[at] + 0.05 * own * own


def moments(count, t, *state):
    nzh, tiles = t.shape[0], t.shape[1] - 3
    shape = jax.ShapeDtypeStruct(state[0].shape, jnp.float32)
    return pl.pallas_call(
        moments_kernel,
        out_shape=(
            jax.ShapeDtypeStruct((count, tiles, nzh, LANES), jnp.bfloat16),
            shape,
            shape,
            shape,
            shape,
        ),
        in_specs=[VMEM] * 5,
        out_specs=(VMEM,) * 5,
        scratch_shapes=[pltpu.VMEM((3, nzh * tiles, LANES), jnp.float32)],
        name="moments",
        compiler_params=params(2),
        cost_estimate=cost(300_000, 400_000),
    )(t, *state)


def total_kernel(d, gram, out, whole):
    tiles = d.shape[1]
    half = tiles // 2
    rows = out.shape[1] // 2
    for f in range(2):
        part = jnp.concatenate(
            [d[:, k].reshape(R, LANES) for k in range(f * half, (f + 1) * half)], axis=1
        )
        whole[f] = part
        square = part.astype(jnp.float32) * (dot(gram[f, 0], part) + dot(gram[f, 1], part))
        out[:, f * rows : (f + 1) * rows] = jnp.full(
            (out.shape[0], rows, LANES), jnp.sum(square)
        )


def totals_of(count, d, gram):
    tiles = d.shape[1]
    cols = tiles // 2 * LANES
    return pl.pallas_call(
        total_kernel,
        out_shape=(
            jax.ShapeDtypeStruct((count, 8, LANES), jnp.float32),
            pltpu.VMEM((2, R, cols), jnp.bfloat16),
        ),
        in_specs=[VMEM, VMEM],
        out_specs=(VMEM, VMEM),
        name="totals",
        compiler_params=params(6),
        cost_estimate=cost(8 * R * R * cols, 2_000_000),
    )(d, *near(gram))


def assemble_kernel(*refs):
    (*whole, _, out) = refs
    zl, x = lax.axis_index("z") % NZL, lax.axis_index("x")
    nzh, nzl, nx = out.shape[:3]
    first = FIRST
    parts = [(k, s, part.at[s]) for k, part in enumerate(whole) for s in range(nzl)]
    for k, s, part in parts:
        px = lax.rem(x + nx - k, nx)
        at = lax.bitwise_xor(zl, s)
        for t in range(part.shape[1]):
            lanes = slice(t * LANES, (t + 1) * LANES)
            out[first:, at, px, :, lanes] = part[: nzh - first, t]
            out[:first, at, px, :, lanes] = part[nzh - first :, t]


def assembled(parts, sizes, after):
    nzh, nzl, nx, _ = sizes
    tiles, rows = parts[0].shape[2:4]
    shape = (nzh, nzl, nx, rows, tiles * LANES)
    return pl.pallas_call(
        assemble_kernel,
        out_shape=jax.ShapeDtypeStruct(shape, jnp.bfloat16),
        in_specs=[VMEM] * len(parts) + [pl.BlockSpec(memory_space=pl.ANY)],
        out_specs=VMEM,
        name="assemble",
        compiler_params=params(8),
        cost_estimate=cost(1_000_000, 4_000_000),
    )(*near(*parts), after)


def final_kernel(totals, directions, factors, mine, other, ov, oo, *refs):
    copy_v, copy_o, sv, so, nv, no, out_v, out_o, own, sems = refs
    steps, nzl, nx, nc, rows, _ = factors.shape[1:]
    chunk = D // steps
    cols = directions.shape[2]
    sums = jnp.sum(totals[...], axis=0)
    scale = lax.rsqrt(sums / (D * WIDTH) + 1e-06)
    scales = scale[:1, :1], scale[4:5, :1]
    writes = []
    for k in range(2):
        part = pl.ds(k * steps // 2, steps // 2)
        lanes = pl.ds(k * D // 2, D // 2)
        writes += [
            pltpu.make_async_copy(out_v.at[part], copy_v.at[part], sems.at[2 * k]),
            pltpu.make_async_copy(out_o.at[:, lanes], copy_o.at[:, lanes], sems.at[2 * k + 1]),
        ]

    z, x, c = (lax.axis_index(a) for a in FS)
    small = []
    for f, (w, targets) in enumerate(((ov, (sv, nv)), (oo, (so, no)))):
        factor = factors[f, z // NZL, z % NZL, x, c]
        step = dot(factor, directions[f]) * scales[f]
        own[2 * f] = step
        own[2 * f + 1] = w[...] - 0.02 * step
        small += [
            pltpu.make_async_copy(own.at[2 * f + k], target, sems.at[4 + 2 * f + k])
            for k, target in enumerate(targets)
        ]
    for copy in small:
        copy.start()

    def copies(pair):
        for i in range(steps):
            for k in range(nc):
                factor = factors[0, i, :, :, k].reshape(chunk // nc, R)
                update = dot(factor, directions[0]) * (0.02 * scales[0])
                w = pair[k][i, :, :, :, :cols].reshape(chunk // nc, cols).astype(jnp.float32)
                out_v[i, :, :, k] = (w - update).astype(jnp.bfloat16).reshape(nzl, nx, rows, cols)
            if (i + 1) * 2 % steps == 0:
                writes[(i + 1) * 4 // steps - 2].start()
            update = dot(factors[1, i].reshape(chunk, R), directions[1]) * (0.02 * scales[1])
            w = jnp.stack([p[i, :, :, :, cols:] for p in pair], axis=2).reshape(chunk, cols)
            half = (w.astype(jnp.float32) - update).astype(jnp.bfloat16)
            out_o[:, i * chunk : (i + 1) * chunk] = half.T
            if (i + 1) * 2 % steps == 0:
                writes[(i + 1) * 4 // steps - 1].start()

    first = c == 0

    @pl.when(first)
    def _():
        copies((mine, other))

    @pl.when(jnp.logical_not(first))
    def _():
        copies((other, mine))

    for copy in small + writes:
        copy.wait()


def final(totals, directions, factors, mine, other, ov, oo):
    cols = directions.shape[2]
    own = pltpu.HBM(ov.shape, jnp.float32)
    shape = (*factors.shape[1:-1], cols)
    copy_value, *rest = pl.pallas_call(
        final_kernel,
        out_shape=(
            pltpu.HBM(shape, jnp.bfloat16),
            pltpu.HBM((cols, D), jnp.bfloat16),
            own,
            own,
            own,
            own,
        ),
        in_specs=[VMEM] * 7,
        out_specs=(HBM,) * 6,
        scratch_shapes=[
            pltpu.VMEM(shape, jnp.bfloat16),
            pltpu.VMEM((cols, D), jnp.bfloat16),
            pltpu.VMEM((4, *ov.shape), jnp.float32),
            pltpu.SemaphoreType.DMA((8,)),
        ],
        name="final",
        compiler_params=params(12),
        cost_estimate=cost(4 * D * cols * R, 10_000_000),
    )(totals, *near(directions, factors, mine, other), ov, oo)
    return copy_value.reshape(D, cols), *rest


def step(
    normed_input,
    value_cotangent,
    gated_output,
    layer_cotangent,
    factor_value,
    factor_output,
    weight_value,
    weight_output,
    first_value,
    second_value,
    first_output,
    second_output,
):
    nz, nx, nc = (lax.axis_size(a) for a in FS)
    nzh, nzl = nz // NZL, NZL
    sizes = nzh, nzl, nx, nc
    ny = lax.axis_size("tp")
    over_xy, over_xc, over_y = plane_groups(nx, nc, ny)
    over_block = block_groups(nz, nx, nc, ny)
    _, cols = weight_value.shape

    turned_weight = weight_output.T
    w = packed(nzh, factor_value, factor_output, weight_value, turned_weight)
    w = exchange(w, "z", far_z(nz))
    f = to_all(w[:, 0], "z", near_z(nz))
    f = to_all(f, PLANE, over_xy)
    other = moved(f, "c", 1)

    get = swapped(w, "z", 1)
    w = jnp.stack([w, get])
    get = swapped(w, "z", 2)
    w0 = jnp.concatenate([w[:, :, 1:], get[:, :, 1:]])

    terms, factors = projected_terms(
        f, other, normed_input, value_cotangent, layer_cotangent, gated_output, sizes
    )
    t = exchange(terms, PLANE, over_xc)
    t = summed(t, nzh)
    w1 = moved(w0, "x", 1)
    w3 = moved(w0, "x", nx - 1)
    t = exchange(t, "z", near_z(nz))

    narrow = (cols // LANES, LANES)
    state = [s.reshape(narrow) for s in (first_value, second_value, first_output, second_output)]
    t = shared(t, *state)
    t = exchange(t, "z", far_z(nz))
    w2 = moved(w1, "x", 1)
    gram = gram_of(factors)
    d, *state = moments(nzl * nx, t, *state)
    next_first_value, next_second_value, next_first_output, next_second_output = (
        s.reshape(1, cols) for s in state
    )
    d = exchange(d, ALL, over_block)
    d = lax.all_gather(d, "c", axis=0, tiled=True)
    mine = assembled((w0, w1, w2, w3), sizes, d)
    flip = moved(mine, "c", 1)

    totals, directions = totals_of(ny, d, gram)
    totals = exchange(totals, PLANE, over_y)

    copy_value, copy_output, step_value, step_output, next_value, next_output = final(
        totals,
        directions,
        factors,
        mine,
        flip,
        weight_value,
        turned_weight,
    )
    return (
        step_value,
        step_output.T,
        next_value,
        next_output.T,
        next_first_value,
        next_second_value,
        next_first_output,
        next_second_output,
        copy_value,
        copy_output,
    )


def solution(mesh):
    torus = Mesh(mesh.devices.reshape(32, 4, 2, mesh.shape["tp"]), ("z", "x", "c", "tp"))
    placed = (
        P(FS, None),
        P(FS, "tp"),
        P(FS, "tp"),
        P(FS, None),
        P(FS, None),
        P(FS, None),
        P(FS, "tp"),
        P("tp", FS),
        P(FS, "tp"),
        P(FS, "tp"),
        P(FS, "tp"),
        P(FS, "tp"),
    )
    return jax.shard_map(
        step,
        mesh=torus,
        in_specs=placed,
        out_specs=(
            P(FS, "tp"),
            P("tp", FS),
            P(FS, "tp"),
            P("tp", FS),
            P(FS, "tp"),
            P(FS, "tp"),
            P(FS, "tp"),
            P(FS, "tp"),
            P(None, "tp"),
            P("tp", None),
        ),
        check_vma=False,
    )
```

```python
import jax
import jax.numpy as jnp
from jax import lax
from jax.experimental import pallas as pl
from jax.experimental.pallas import tpu as pltpu
from jax.sharding import Mesh
from jax.sharding import PartitionSpec as P

D = 2048
WIDTH = 2048
R = 256
FS = ("z", "x", "c")
PLANE = ("x", "c", "tp")
ALL = ("z", *PLANE)
NZL = 4
FIRST = 5
LANES = 128
TN = (((0,), (0,)), ((), ()))


VMEM = pl.BlockSpec(memory_space=pltpu.VMEM)
HBM = pl.BlockSpec(memory_space=pltpu.HBM)


def far(*arrays):
    return [pltpu.with_memory_space_constraint(a, pltpu.HBM) for a in arrays]


def near(*arrays):
    return [pltpu.with_memory_space_constraint(a, pltpu.VMEM) for a in arrays]


def params(mib):
    return pltpu.CompilerParams(vmem_limit_bytes=mib << 20)


def cost(flops, bytes_accessed):
    return pl.CostEstimate(flops=flops, bytes_accessed=bytes_accessed, transcendentals=0)


def dot(a, b, dims=(((1,), (0,)), ((), ()))):
    return lax.dot_general(a, b, dims, preferred_element_type=jnp.float32)


def turned(n, by):
    return [(i + by) % n for i in range(n)]


def near_z(nz):
    return [[i + k for k in (1, 0, 2, 3)] for i in range(0, nz, NZL)]


def far_z(nz):
    n = nz // NZL
    return [[i + NZL * k for k in turned(n, FIRST)] for i in range(NZL)]


def plane_groups(nx, nc, ny):
    xs, ys = turned(nx, nx // 2), turned(ny, ny // 2)
    at = lambda x, c, y: (x * nc + c) * ny + y
    return (
        [[at(x, c, y) for x in xs for y in ys] for c in range(nc)],
        [[at(x, c, y) for c in range(nc) for x in xs] for y in range(ny)],
        [[at(x, c, y) for y in ys] for x in range(nx) for c in range(nc)],
    )


def block_groups(nz, nx, nc, ny):
    return [
        [((z * nx + x) * nc + c) * ny + y for x in turned(nx, nx // 2) for z in near]
        for near in near_z(nz)
        for c in range(nc)
        for y in range(ny)
    ]


def column_of(k, nzh):
    slot = k // nzh % NZL
    near = jnp.where(slot < 2, 1 - slot, slot)
    z = (k % nzh + FIRST) % nzh * NZL + near
    place = k // (nzh * NZL)
    return z * 8 + (place + 2) % 4 * 2 + place // 4


def exchange(blocks, axes, groups=None):
    return lax.all_to_all(
        blocks, axes, split_axis=0, concat_axis=0, axis_index_groups=groups, tiled=True
    )


def to_all(block, axes, groups=None):
    count = len(groups[0]) if groups else lax.axis_size(axes)
    copies = jnp.broadcast_to(block[None], (count, *block.shape))
    return exchange(copies, axes, groups)


def moved(block, axis, by):
    n = lax.axis_size(axis)
    return lax.ppermute(block, axis, [(i, (i + by) % n) for i in range(n)])


def swapped(block, axis, bit):
    return lax.ppermute(block, axis, [(i, i ^ bit) for i in range(lax.axis_size(axis))])


def pack_kernel(fv, fo, wv, wo, out, fv_in, fo_in, wv_in, wo_in, sems):
    copies = [
        pltpu.make_async_copy(src, dst, sems.at[i])
        for i, (src, dst) in enumerate(((fv, fv_in), (fo, fo_in), (wv, wv_in), (wo, wo_in)))
    ]
    for copy in copies:
        copy.start()
    n = R // 8
    y = lax.axis_index("tp")
    j = lax.broadcasted_iota(jnp.int32, (R, R), 0)
    k = lax.broadcasted_iota(jnp.int32, (R, R), 1)
    turn = (j == column_of(k, n // NZL)).astype(jnp.bfloat16)
    for copy in copies:
        copy.wait()
    factor = jnp.where(y < 2, fv_in[...].astype(jnp.float32), fo_in[...].astype(jnp.float32))
    factor = dot(factor.astype(jnp.bfloat16), turn)
    tile = jnp.where(y % 2 == 0, factor[:, :LANES], factor[:, LANES:]).astype(jnp.bfloat16)
    tiles = [tile]
    for w in (wv_in, wo_in):
        half = w[...].astype(jnp.bfloat16)
        tiles += [half[:, t : t + LANES] for t in range(0, half.shape[1], LANES)]
    for t, tile in enumerate(tiles):
        out[:, t] = jnp.broadcast_to(tile[None], (out.shape[0], *tile.shape))


def packed(count, fv, fo, wv, wo):
    rows, cols = wv.shape
    tiles = 1 + 2 * cols // LANES
    return pl.pallas_call(
        pack_kernel,
        out_shape=jax.ShapeDtypeStruct((count, tiles, rows, LANES), jnp.bfloat16),
        in_specs=[HBM] * 4,
        out_specs=VMEM,
        scratch_shapes=[
            pltpu.VMEM(fv.shape, fv.dtype),
            pltpu.VMEM(fo.shape, fo.dtype),
            pltpu.VMEM(wv.shape, wv.dtype),
            pltpu.VMEM(wo.shape, wo.dtype),
            pltpu.SemaphoreType.DMA((4,)),
        ],
        name="packed",
        compiler_params=params(4),
        cost_estimate=cost(2 * 8 * R * R, 200_000),
    )(*far(fv, fo, wv, wo))


def project_kernel(mine, other, xv, vv, xo, vo, keep, give, whole, late, sems):
    c = lax.axis_index("c")
    read = pltpu.make_async_copy(xo, late, sems.at[0])
    read.start()
    nzh, nzl, nx = whole.shape[1:4]
    first = FIRST
    half = R // LANES
    cols = vv.shape[1]
    for f in range(2):
        for src, at in ((mine, c), (other, 1 - c)):
            for x in range(nx):
                for h in range(half):
                    for k, zl in enumerate(near_z(nzl)[0]):
                        lanes = slice(h * LANES, (h + 1) * LANES)
                        y = (f * half + h + half) % (2 * half)
                        block = src.at[(x + nx // 2) % nx * 2 * half + y, k]
                        whole[f, first:, zl, x, at, :, lanes] = block[: nzh - first]
                        whole[f, :first, zl, x, at, :, lanes] = block[nzh - first :]
    for f, (x, v) in enumerate(((xv, vv), (late, vo))):
        if f == 1:
            read.wait()
        projected = dot(x[...], whole[f].reshape(D, R)).astype(jnp.bfloat16)
        term = dot(projected, v[...], TN).astype(jnp.bfloat16)
        term = term.reshape(2, *keep.shape[:2], cols)
        lanes = slice(f * cols, (f + 1) * cols)
        keep[:, :, lanes] = jnp.where(c == 0, term[0], term[1])
        give[:, :, lanes] = jnp.where(c == 0, term[1], term[0])


def projected_terms(mine, other, xv, vv, xo, vo, sizes):
    nzh, nzl, nx, nc = sizes
    shape = (2, nzh, nzl, nx, nc, D // (nzh * nzl * nx * nc), R)
    cols = vv.shape[1]
    tokens = xv.shape[0]
    return pl.pallas_call(
        project_kernel,
        out_shape=(
            jax.ShapeDtypeStruct((nx, nzh * nzl, 2 * cols), jnp.bfloat16),
            jax.ShapeDtypeStruct((nx, nzh * nzl, 2 * cols), jnp.bfloat16),
            pltpu.VMEM(shape, jnp.bfloat16),
        ),
        in_specs=[VMEM] * 4 + [HBM, VMEM],
        out_specs=(VMEM,) * 3,
        scratch_shapes=[pltpu.VMEM(xo.shape, xo.dtype), pltpu.SemaphoreType.DMA((1,))],
        name="project",
        compiler_params=params(12),
        cost_estimate=cost(4 * tokens * R * (D + cols), 10_000_000),
    )(mine, other, *near(xv, vv), *far(xo), *near(vo))


def paired_kernel(keep, get, out):
    total = keep[...].astype(jnp.float32) + get[...].astype(jnp.float32)
    out[...] = total.astype(jnp.bfloat16)


def paired(keep, get):
    return pl.pallas_call(
        paired_kernel,
        out_shape=jax.ShapeDtypeStruct(keep.shape, jnp.bfloat16),
        in_specs=[VMEM, VMEM],
        out_specs=VMEM,
        name="paired",
        compiler_params=params(2),
        cost_estimate=cost(keep.size, 800_000),
    )(keep, get)


def shared_kernel(t, fv, sv, fo, so, out):
    total = jnp.sum(t[...].astype(jnp.float32), axis=0)
    tiles = total.shape[1] // LANES
    first = 0.9 * jnp.concatenate([fv[...], fo[...]], axis=0)
    high = first.astype(jnp.bfloat16)
    low = (first - high.astype(jnp.float32)).astype(jnp.bfloat16)
    second = (0.95 * jnp.concatenate([sv[...], so[...]], axis=0)).astype(jnp.bfloat16)
    blocks = [total[:, k * LANES : (k + 1) * LANES].astype(jnp.bfloat16) for k in range(tiles)]
    for k, block in enumerate([*blocks, high, low, second]):
        out[:, k] = jnp.broadcast_to(block[None], (out.shape[0], *block.shape))


def shared(t, *state):
    _, nzh, width = t.shape
    shape = (nzh, width // LANES + 3, nzh, LANES)
    return pl.pallas_call(
        shared_kernel,
        out_shape=jax.ShapeDtypeStruct(shape, jnp.bfloat16),
        in_specs=[VMEM] * 5,
        out_specs=VMEM,
        name="shared",
        compiler_params=params(2),
        cost_estimate=cost(t.size, 400_000),
    )(t, *state)


def gram_kernel(factors, grams):
    for f in range(2):
        factor = factors[f].reshape(D, R)
        gram = dot(factor, factor, TN)
        high = gram.astype(jnp.bfloat16)
        grams[f, 0] = high
        grams[f, 1] = (gram - high.astype(jnp.float32)).astype(jnp.bfloat16)


def gram_of(factors):
    shape = (2, 2, R, R)
    return pl.pallas_call(
        gram_kernel,
        out_shape=pltpu.VMEM(shape, jnp.bfloat16),
        in_specs=[VMEM],
        out_specs=VMEM,
        name="gram",
        compiler_params=params(8),
        cost_estimate=cost(4 * D * R * R, 3_000_000),
    )(*near(factors))


def moments_kernel(t, fv, sv, fo, so, out, nfv, nsv, nfo, nso, lines):
    nzh = t.shape[0]
    tiles = t.shape[1] - 3
    states = []
    for k in range(3):
        lines[k] = t[:, tiles + k].astype(jnp.float32).reshape(nzh * tiles, LANES)
        states.append([lines[k, pl.ds(s, nzh, stride=tiles), :] for s in range(tiles)])
    mine = lax.rem(lax.axis_index("z") // NZL + nzh - FIRST, nzh)
    here = lax.broadcasted_iota(jnp.int32, (nzh, LANES), 0) == mine
    half = tiles // 2
    for k in range(tiles):
        low = jnp.sum(t[:, k].astype(jnp.float32), axis=0)
        first = states[0][k] + states[1][k] + 0.1 * low
        second = states[2][k] + 0.05 * low * low
        d = (first * lax.rsqrt(second)).astype(jnp.bfloat16)
        out[:, k] = jnp.broadcast_to(d[None], (out.shape[0], *d.shape))
        own = jnp.sum(jnp.where(here, low, 0.0), axis=0, keepdims=True)
        at = slice(k % half, k % half + 1)
        f, s, nf, ns = (fv, sv, nfv, nsv) if k < half else (fo, so, nfo, nso)
        nf[at] = 0.9 * f[at] + 0.1 * own
        ns[at] = 0.95 * s[at] + 0.05 * own * own


def moments(count, t, *state):
    nzh, tiles = t.shape[0], t.shape[1] - 3
    shape = jax.ShapeDtypeStruct(state[0].shape, jnp.float32)
    return pl.pallas_call(
        moments_kernel,
        out_shape=(
            jax.ShapeDtypeStruct((count, tiles, nzh, LANES), jnp.bfloat16),
            shape,
            shape,
            shape,
            shape,
        ),
        in_specs=[VMEM] * 5,
        out_specs=(VMEM,) * 5,
        scratch_shapes=[pltpu.VMEM((3, nzh * tiles, LANES), jnp.float32)],
        name="moments",
        compiler_params=params(2),
        cost_estimate=cost(300_000, 400_000),
    )(t, *state)


def total_kernel(d, gram, out, whole):
    tiles = d.shape[1]
    half = tiles // 2
    rows = out.shape[1] // 2
    for f in range(2):
        part = jnp.concatenate(
            [d[:, k].reshape(R, LANES) for k in range(f * half, (f + 1) * half)], axis=1
        )
        whole[f] = part
        square = part.astype(jnp.float32) * (dot(gram[f, 0], part) + dot(gram[f, 1], part))
        out[:, f * rows : (f + 1) * rows] = jnp.full(
            (out.shape[0], rows, LANES), jnp.sum(square)
        )


def totals_of(count, d, gram):
    tiles = d.shape[1]
    cols = tiles // 2 * LANES
    return pl.pallas_call(
        total_kernel,
        out_shape=(
            jax.ShapeDtypeStruct((count, 8, LANES), jnp.float32),
            pltpu.VMEM((2, R, cols), jnp.bfloat16),
        ),
        in_specs=[VMEM, VMEM],
        out_specs=(VMEM, VMEM),
        name="totals",
        compiler_params=params(6),
        cost_estimate=cost(8 * R * R * cols, 2_000_000),
    )(d, *near(gram))


def assemble_kernel(*refs):
    (*whole, _, out) = refs
    zl, x = lax.axis_index("z") % NZL, lax.axis_index("x")
    nzh, nzl, nx = out.shape[:3]
    first = FIRST
    parts = [(k, s, part.at[s]) for k, part in enumerate(whole) for s in range(nzl)]
    for k, s, part in parts:
        px = lax.rem(x + nx - k, nx)
        at = lax.bitwise_xor(zl, s)
        for t in range(part.shape[1]):
            lanes = slice(t * LANES, (t + 1) * LANES)
            out[first:, at, px, :, lanes] = part[: nzh - first, t]
            out[:first, at, px, :, lanes] = part[nzh - first :, t]


def assembled(parts, sizes, after):
    nzh, nzl, nx, _ = sizes
    tiles, rows = parts[0].shape[2:4]
    shape = (nzh, nzl, nx, rows, tiles * LANES)
    return pl.pallas_call(
        assemble_kernel,
        out_shape=jax.ShapeDtypeStruct(shape, jnp.bfloat16),
        in_specs=[VMEM] * len(parts) + [pl.BlockSpec(memory_space=pl.ANY)],
        out_specs=VMEM,
        name="assemble",
        compiler_params=params(8),
        cost_estimate=cost(1_000_000, 4_000_000),
    )(*near(*parts), after)


def final_kernel(totals, directions, factors, mine, other, ov, oo, *refs):
    copy_v, copy_o, sv, so, nv, no, out_v, out_o, own, sems = refs
    steps, nzl, nx, nc, rows, _ = factors.shape[1:]
    chunk = D // steps
    cols = directions.shape[2]
    sums = jnp.sum(totals[...], axis=0)
    scale = lax.rsqrt(sums / (D * WIDTH) + 1e-06)
    scales = scale[:1, :1], scale[4:5, :1]
    writes = []
    for k in range(2):
        part = pl.ds(k * steps // 2, steps // 2)
        lanes = pl.ds(k * D // 2, D // 2)
        writes += [
            pltpu.make_async_copy(out_v.at[part], copy_v.at[part], sems.at[2 * k]),
            pltpu.make_async_copy(out_o.at[:, lanes], copy_o.at[:, lanes], sems.at[2 * k + 1]),
        ]

    z, x, c = (lax.axis_index(a) for a in FS)
    small = []
    for f, (w, targets) in enumerate(((ov, (sv, nv)), (oo, (so, no)))):
        factor = factors[f, z // NZL, z % NZL, x, c]
        step = dot(factor, directions[f]) * scales[f]
        own[2 * f] = step
        own[2 * f + 1] = w[...] - 0.02 * step
        small += [
            pltpu.make_async_copy(own.at[2 * f + k], target, sems.at[4 + 2 * f + k])
            for k, target in enumerate(targets)
        ]
    for copy in small:
        copy.start()

    def copies(pair):
        for i in range(steps):
            for k in range(nc):
                factor = factors[0, i, :, :, k].reshape(chunk // nc, R)
                update = dot(factor, directions[0]) * (0.02 * scales[0])
                w = pair[k][i, :, :, :, :cols].reshape(chunk // nc, cols).astype(jnp.float32)
                out_v[i, :, :, k] = (w - update).astype(jnp.bfloat16).reshape(nzl, nx, rows, cols)
            if (i + 1) * 2 % steps == 0:
                writes[(i + 1) * 4 // steps - 2].start()
            update = dot(factors[1, i].reshape(chunk, R), directions[1]) * (0.02 * scales[1])
            w = jnp.stack([p[i, :, :, :, cols:] for p in pair], axis=2).reshape(chunk, cols)
            half = (w.astype(jnp.float32) - update).astype(jnp.bfloat16)
            out_o[:, i * chunk : (i + 1) * chunk] = half.T
            if (i + 1) * 2 % steps == 0:
                writes[(i + 1) * 4 // steps - 1].start()

    first = c == 0

    @pl.when(first)
    def _():
        copies((mine, other))

    @pl.when(jnp.logical_not(first))
    def _():
        copies((other, mine))

    for copy in small + writes:
        copy.wait()


def final(totals, directions, factors, mine, other, ov, oo):
    cols = directions.shape[2]
    own = pltpu.HBM(ov.shape, jnp.float32)
    shape = (*factors.shape[1:-1], cols)
    copy_value, *rest = pl.pallas_call(
        final_kernel,
        out_shape=(
            pltpu.HBM(shape, jnp.bfloat16),
            pltpu.HBM((cols, D), jnp.bfloat16),
            own,
            own,
            own,
            own,
        ),
        in_specs=[VMEM] * 7,
        out_specs=(HBM,) * 6,
        scratch_shapes=[
            pltpu.VMEM(shape, jnp.bfloat16),
            pltpu.VMEM((cols, D), jnp.bfloat16),
            pltpu.VMEM((4, *ov.shape), jnp.float32),
            pltpu.SemaphoreType.DMA((8,)),
        ],
        name="final",
        compiler_params=params(12),
        cost_estimate=cost(4 * D * cols * R, 10_000_000),
    )(totals, *near(directions, factors, mine, other), ov, oo)
    return copy_value.reshape(D, cols), *rest


def step(
    normed_input,
    value_cotangent,
    gated_output,
    layer_cotangent,
    factor_value,
    factor_output,
    weight_value,
    weight_output,
    first_value,
    second_value,
    first_output,
    second_output,
):
    nz, nx, nc = (lax.axis_size(a) for a in FS)
    nzh, nzl = nz // NZL, NZL
    sizes = nzh, nzl, nx, nc
    ny = lax.axis_size("tp")
    over_xy, _, over_y = plane_groups(nx, nc, ny)
    over_block = block_groups(nz, nx, nc, ny)
    _, cols = weight_value.shape

    turned_weight = weight_output.T
    w = packed(nzh, factor_value, factor_output, weight_value, turned_weight)
    w = exchange(w, "z", far_z(nz))
    f = to_all(w[:, 0], "z", near_z(nz))
    f = to_all(f, PLANE, over_xy)
    other = moved(f, "c", 1)

    get = swapped(w, "z", 1)
    w = jnp.stack([w, get])
    get = swapped(w, "z", 2)
    w0 = jnp.concatenate([w[:, :, 1:], get[:, :, 1:]])

    keep, give, factors = projected_terms(
        f, other, normed_input, value_cotangent, layer_cotangent, gated_output, sizes
    )
    across = moved(give, "c", 1)
    t = paired(keep, across)
    t = exchange(t.reshape(nx * nzl, nzh, 2 * cols), ALL, over_block)
    w1 = moved(w0, "x", 1)
    w3 = moved(w0, "x", nx - 1)
    narrow = (cols // LANES, LANES)
    state = [s.reshape(narrow) for s in (first_value, second_value, first_output, second_output)]
    t = shared(t, *state)
    t = exchange(t, "z", far_z(nz))
    w2 = moved(w1, "x", 1)
    gram = gram_of(factors)
    d, *state = moments(nzl * nx, t, *state)
    next_first_value, next_second_value, next_first_output, next_second_output = (
        s.reshape(1, cols) for s in state
    )
    d = exchange(d, ALL, over_block)
    d = lax.all_gather(d, "c", axis=0, tiled=True)
    mine = assembled((w0, w1, w2, w3), sizes, d)
    flip = moved(mine, "c", 1)

    totals, directions = totals_of(ny, d, gram)
    totals = exchange(totals, PLANE, over_y)

    copy_value, copy_output, step_value, step_output, next_value, next_output = final(
        totals,
        directions,
        factors,
        mine,
        flip,
        weight_value,
        turned_weight,
    )
    return (
        step_value,
        step_output.T,
        next_value,
        next_output.T,
        next_first_value,
        next_second_value,
        next_first_output,
        next_second_output,
        copy_value,
        copy_output,
    )


def solution(mesh):
    torus = Mesh(mesh.devices.reshape(32, 4, 2, mesh.shape["tp"]), ("z", "x", "c", "tp"))
    placed = (
        P(FS, None),
        P(FS, "tp"),
        P(FS, "tp"),
        P(FS, None),
        P(FS, None),
        P(FS, None),
        P(FS, "tp"),
        P("tp", FS),
        P(FS, "tp"),
        P(FS, "tp"),
        P(FS, "tp"),
        P(FS, "tp"),
    )
    return jax.shard_map(
        step,
        mesh=torus,
        in_specs=placed,
        out_specs=(
            P(FS, "tp"),
            P("tp", FS),
            P(FS, "tp"),
            P("tp", FS),
            P(FS, "tp"),
            P(FS, "tp"),
            P(FS, "tp"),
            P(FS, "tp"),
            P(None, "tp"),
            P("tp", None),
        ),
        check_vma=False,
    )
```
